32 devices in a mesh: ep: 8 (over z, x), tp: 4 (over y, core).
Axes of the slice: x: 2, y: 2, z: 4, core: 2. Of those that a mesh axis runs over, the one named last changes fastest.
Arguments:
- query_in: bfloat16 [4096, 2048], P('ep', 'tp'), may hold values from -6 to 6
- key_in: bfloat16 [4096, 2048], P('ep', 'tp'), may hold values from -6 to 6
- value_in: bfloat16 [4096, 2048], P('ep', 'tp'), may hold values from -6 to 6
- gate_in: bfloat16 [4096, 2048], P('ep', 'tp'), may hold values from -6 to 6
- decay_rate: float32 [16], P('tp'), may hold values from 0 to 0.04
- head_gain: float32 [2048], P('tp'), may hold values from 0.1 to 1.9
- output_weight: bfloat16 [2048, 2048], P('tp'), may hold values from -0.125 to 0.125
- token_rows: bfloat16 [1536, 2048], P('ep'), may hold values from -100 to 100
- token_gain: float32 [2048], replicated, may hold values from 0.1 to 1.9
- route_ids: int32 [1536, 2], P('ep'), may hold values from 0 to 7, all different within a row; in each aligned block of 192 rows (0 to 191, 192 to 383, ...) at most 96 rows name the same one
- route_weights: float32 [1536, 2], P('ep'), may hold values from 0.25 to 2.5
- expert_gate: bfloat16 [8, 2048, 4096], P('ep', None, 'tp'), may hold values from -0.125 to 0.125
- expert_up: bfloat16 [8, 2048, 4096], P('ep', None, 'tp'), may hold values from -0.125 to 0.125
- expert_down: bfloat16 [8, 4096, 2048], P('ep', None, 'tp'), may hold values from -0.09375 to 0.09375
Outputs:
- retained_out: bfloat16 [4096, 2048], P(('ep', 'tp'))
- expert_out: bfloat16 [1536, 2048], P('ep', 'tp')
The draws below stay inside these ranges and needn't reach their ends.
Inputs may be any that keep to these rules, and one draw needn't show every extreme that they name: `route_ids`: each row names 2 different experts. In each aligned block of 192 rows (the rows of one index of ep) no expert is named by more than 96 rows, a bound that some block reaches.
All inputs are finite; a program needn't handle non-finite values.
Results may differ from the reference program's by a relative error of at most 0.019.
Values may be sent and summed in bfloat16 or wider, within the bound.
A program may use at most 64 MiB of HBM per device.

```python
import math
import jax
import jax.numpy as jnp
import numpy as np
from jax import lax

D = 2048
HEADS = 16
DK = 128
DV = 128
FF = 4096
TOP = 2
TOK_MIX = 512
TOK_MOE = 192
EXPERTS = 8
SEQ_MIX = 4096
TOKENS_MOE = 1536
CAP = 96
N_EP = 8
N_TP = 4


def draw_decay_rate(key, part):
    subkeys = jax.random.split(jax.random.fold_in(key, 11), 3)
    fast_share = 0.5
    is_fast = jax.random.uniform(subkeys[0], (HEADS,)) < fast_share
    fast_rate = jnp.exp(jax.random.uniform(subkeys[1], (HEADS,), minval=jnp.log(0.01), maxval=jnp.log(1.0 / 30.0)))
    slow_rate = jnp.exp(jax.random.uniform(subkeys[2], (HEADS,), minval=jnp.log(0.1 / SEQ_MIX), maxval=jnp.log(1.5 / SEQ_MIX)))
    return jnp.where(is_fast, fast_rate, slow_rate).astype(jnp.float32)


def draw_value_in(key, part):
    subkeys = jax.random.split(jax.random.fold_in(key, 37), 2)
    row_scale = jnp.exp(jax.random.uniform(subkeys[0], (SEQ_MIX, 1), minval=jnp.log(0.3), maxval=jnp.log(3.0)))
    base = jnp.clip(jax.random.normal(subkeys[1], (SEQ_MIX, HEADS * DV), jnp.float32), -2.0, 2.0)
    return (base * row_scale).astype(jnp.bfloat16)


def draw_token_rows(key, part):
    subkeys = jax.random.split(jax.random.fold_in(key, 23), 3)
    column_scale = jnp.exp(jax.random.uniform(subkeys[1], (1, D), minval=jnp.log(0.4), maxval=jnp.log(4.0)))
    row_scale = jnp.exp(jax.random.uniform(subkeys[0], (TOKENS_MOE, 1), minval=jnp.log(0.3), maxval=jnp.log(3.0)))
    base = jnp.clip(jax.random.normal(subkeys[2], (TOKENS_MOE, D), jnp.float32), -4.0, 4.0)
    return (base * row_scale * column_scale).astype(jnp.bfloat16)


def steps_of(stream_key, shape, cuts, smallest, top_value):
    loudness = 1.0
    for position, shards_of in cuts:
        heights = jax.random.uniform(jax.random.fold_in(jax.random.fold_in(stream_key, 6), position), (shards_of,), jnp.float32, smallest / len(cuts), top_value / len(cuts))
        loudness = loudness * jnp.repeat(jnp.exp(heights), shape[position] // shards_of).reshape((-1,) + (1,) * (len(shape) - 1 - position))
    return loudness


def shared_out(rng, own, number, rows, number_of, top, most, lean):
    sequence = jax.random.permutation(rng, number_of)
    packed, usual = load_shares(number_of, rows * top, most, lean, True), load_shares(number_of, rows * top, most, lean, False)
    places = jnp.arange(number_of)

    def named(sizes, rotation):
        used = int((sizes > 0).sum())
        fixed = max(1, used // 4)
        moved = fixed + (places - fixed + rotation * (used - fixed)) % max(1, number_of - fixed)
        return jnp.zeros((number_of,), jnp.int32).at[sequence[jnp.where(places < fixed, places, moved)]].set(jnp.asarray(sizes, jnp.int32))

    sizes = jnp.where(number % 4 == 0, named(packed, number // 4), named(usual, number - number // 4 - 1))
    mixed = jax.random.permutation(jax.random.fold_in(own, 3), number_of)
    donor, receiver = mixed[0:number_of // 2 * 2:2], mixed[1:number_of // 2 * 2:2]
    slack = jnp.minimum(sizes[donor] - 1, most - sizes[receiver]) // 2
    slack = jnp.where((donor == sequence[0]) | (receiver == sequence[0]) | (sizes[receiver] == 0), 0, jnp.maximum(slack, 0))
    moved = jax.random.randint(jax.random.fold_in(own, 4), (number_of // 2,), 0, 1 << 20) % (slack + 1)
    sizes = sizes.at[donor].add(-moved).at[receiver].add(moved)
    items = jnp.searchsorted(jnp.cumsum(sizes), jnp.arange(rows * top), side="right").astype(jnp.int32)
    table = items.reshape(top, rows).T
    table = table[jax.random.permutation(jax.random.fold_in(own, 1), rows)]
    rotation = jax.random.randint(jax.random.fold_in(own, 2), (rows, 1), 0, top)
    return jnp.take_along_axis(table, (jnp.arange(top)[None, :] + rotation) % top, axis=1)


def load_shares(count, total, most, slope, full):
    loads = [(1 << 20) // math.isqrt(grade ** slope) + 1 for grade in range(1, count + 1)]
    largest = most if full else min(most, max(-(-total // count), total * loads[0] // sum(loads)))
    least = 1 if total - largest >= count - 1 else 0
    counts, surplus = [largest] + [least] * (count - 1), total - largest - least * (count - 1)
    while surplus > 0:
        candidates = [i for i in range(1, count) if counts[i] < largest] or [i for i in range(1, count) if counts[i] < most]
        mass, budget = sum([loads[i] for i in candidates]), surplus
        for i in candidates:
            addition = min(most - counts[i], max(1, budget * loads[i] // mass), surplus)
            counts[i] = counts[i] + addition
            surplus = surplus - addition
    return np.array(counts)


def gaussian(own_key, dims, deviation, limit, cuts=(), held_as=jnp.bfloat16):
    factor_of = steps_of(own_key, dims, cuts, -0.22, 0.18) if cuts else 1.0
    entries = jax.random.normal(own_key, dims, jnp.float32) * deviation * factor_of
    return jnp.minimum(jnp.maximum(entries, -limit), limit).astype(held_as)


def setup_inputs(seed: int = 0) -> dict:
    keys = jax.random.split(jax.random.key(seed), 15)
    query_in = gaussian(keys[0], (SEQ_MIX, HEADS * DK), 1.0, 6.0, ((0, 8), (1, 4)))
    key_in = gaussian(keys[1], (SEQ_MIX, HEADS * DK), 1.0, 6.0, ((0, 8), (1, 4)))
    value_in = draw_value_in(jax.random.fold_in(keys[14], 71), 0)
    gate_in = gaussian(keys[3], (SEQ_MIX, HEADS * DV), 1.0, 6.0, ((0, 8), (1, 4)))
    decay_rate = draw_decay_rate(jax.random.fold_in(keys[14], 71), 0)
    head_gain = jnp.clip(1.0 + 0.18 * jax.random.normal(keys[5], (HEADS * DV,), jnp.float32), 0.1, 1.9)
    output_weight = gaussian(keys[6], (HEADS * DV, D), (HEADS * DV) ** -0.5, 0.125, ((0, 4),))
    token_rows = draw_token_rows(jax.random.fold_in(keys[14], 71), 0)
    token_gain = jnp.clip(1.0 + 0.18 * jax.random.normal(keys[8], (D,), jnp.float32), 0.1, 1.9)
    route_ids_keys = jax.random.split(jax.random.fold_in(keys[9], 1), TOKENS_MOE // TOK_MOE)
    route_ids_turns = jax.random.permutation(jax.random.fold_in(keys[9], 3), TOKENS_MOE // TOK_MOE)
    route_ids = jax.vmap(lambda own, number: shared_out(jax.random.fold_in(keys[9], 2), own, number, TOK_MOE, EXPERTS, TOP, CAP, 1))(route_ids_keys, route_ids_turns).reshape((TOKENS_MOE, TOP))
    route_weights = jnp.clip(jnp.exp(math.log(2.5) - 2.3025851 * jax.random.uniform(keys[10], (TOKENS_MOE, TOP), jnp.float32) ** steps_of(keys[10], (TOKENS_MOE, TOP), ((0, 8),), -0.2, 0.2)), 0.25, 2.5)
    expert_gate = gaussian(keys[11], (EXPERTS, D, FF), D ** -0.5, 0.125, ((0, 8), (2, 4)))
    expert_up = gaussian(keys[12], (EXPERTS, D, FF), D ** -0.5, 0.125, ((0, 8), (2, 4)))
    expert_down = gaussian(keys[13], (EXPERTS, FF, D), FF ** -0.5, 0.09375, ((0, 8), (2, 4)))
    return dict(query_in=query_in, key_in=key_in, value_in=value_in, gate_in=gate_in, decay_rate=decay_rate, head_gain=head_gain, output_weight=output_weight, token_rows=token_rows, token_gain=token_gain, route_ids=route_ids, route_weights=route_weights, expert_gate=expert_gate, expert_up=expert_up, expert_down=expert_down)


epsilon = 1e-06
rope_base = 10000.0

def rotate(values, positions):
    half_dim = values.shape[-1] // 2
    frequency = rope_base ** (-jnp.arange(half_dim, dtype=jnp.float32) * 2.0 / values.shape[-1])
    angles = positions.astype(jnp.float32)[:, None] * frequency[None, :]
    cosine_table = jnp.cos(angles)[:, None, :]
    sine_table = jnp.sin(angles)[:, None, :]
    first_half = values[..., :half_dim]
    second = values[..., half_dim:]
    return jnp.concatenate([first_half * cosine_table - second * sine_table, second * cosine_table + first_half * sine_table], -1)

def retention(query_in, key_in, value_in, gate_in, decay_rate, head_gain, output_weight):
    seq_length = query_in.shape[0]
    blocks = seq_length // TOK_MIX
    head_count = decay_rate.shape[0]
    highest = lax.Precision.HIGHEST
    positions = jnp.arange(seq_length, dtype=jnp.int32)
    rot_query = rotate(query_in.astype(jnp.float32).reshape(seq_length, head_count, DK), positions).astype(jnp.bfloat16)
    rot_key = (rotate(key_in.astype(jnp.float32).reshape(seq_length, head_count, DK), positions) * DK ** (-0.5)).astype(jnp.bfloat16)
    value_heads = value_in.reshape(seq_length, head_count, DV)
    within = jnp.arange(TOK_MIX, dtype=jnp.float32)
    distance = within[:, None] - within[None, :]
    decay_mat = jnp.where(distance[None] >= 0, jnp.exp(-decay_rate[:, None, None] * jnp.maximum(distance, 0.0)[None]), 0.0)
    key_decay = jnp.exp(-decay_rate[None, :] * (TOK_MIX - 1.0 - within)[:, None])
    query_decay = jnp.exp(-decay_rate[None, :] * (within + 1.0)[:, None])
    span_decay = jnp.exp(-decay_rate * TOK_MIX)

    def one_block(pieces):
        query_block, key_block, value_block = pieces
        scores = jnp.einsum('ihd,jhd->hij', query_block.astype(jnp.float32), key_block.astype(jnp.float32), precision=highest)
        weights = (scores * decay_mat).astype(jnp.bfloat16)
        local_out = jnp.einsum('hij,jhe->ihe', weights.astype(jnp.float32), value_block.astype(jnp.float32), precision=highest)
        decayed = (key_block.astype(jnp.float32) * key_decay[:, :, None]).astype(jnp.bfloat16)
        block_state = jnp.einsum('jhd,jhe->hde', decayed.astype(jnp.float32), value_block.astype(jnp.float32), precision=highest)
        return (local_out, block_state)
    query_blocks = rot_query.reshape(blocks, TOK_MIX, head_count, DK)
    local_out, states = lax.map(one_block, (query_blocks, rot_key.reshape(blocks, TOK_MIX, head_count, DK), value_heads.reshape(blocks, TOK_MIX, head_count, DV)))

    def carry_step(running, block_state):
        return (running * span_decay[:, None, None] + block_state, running)
    initial = jnp.zeros((head_count, DK, DV), jnp.float32)
    final_state, carried = lax.scan(carry_step, initial, states)
    carried_out = jnp.einsum('bihd,bhde->bihe', query_blocks.astype(jnp.float32), carried, precision=highest) * query_decay[None, :, :, None]
    retained = (local_out + carried_out).reshape(seq_length, head_count, DV)
    centered = retained - lax.optimization_barrier(jnp.mean(retained, -1, keepdims=True))
    normed = centered * lax.rsqrt(lax.optimization_barrier(jnp.mean(centered * centered, -1, keepdims=True)) + epsilon)
    mixed = (normed.reshape(seq_length, head_count * DV) * head_gain * jax.nn.silu(gate_in.astype(jnp.float32))).astype(jnp.bfloat16)
    group_width = head_count // N_TP * DV

    def add_group(group_index, summed):
        first_col = (group_index * group_width).astype(jnp.int32)
        columns = lax.dynamic_slice_in_dim(mixed, first_col, group_width, 1)
        weight_rows = lax.dynamic_slice_in_dim(output_weight, first_col, group_width, 0)
        group_part = jnp.dot(columns, weight_rows, preferred_element_type=jnp.float32).astype(jnp.bfloat16)
        return summed + lax.optimization_barrier(group_part).astype(jnp.float32)
    summed = lax.fori_loop(0, N_TP, add_group, jnp.zeros((seq_length, output_weight.shape[1]), jnp.float32))
    return summed.astype(jnp.bfloat16)

def experts(token_rows, token_gain, route_ids, route_weights, expert_gate, expert_up, expert_down):
    token_count, model_dim = token_rows.shape
    rows_float = token_rows.astype(jnp.float32)
    normed = (rows_float * lax.rsqrt(lax.optimization_barrier(jnp.mean(rows_float * rows_float, -1, keepdims=True)) + epsilon) * token_gain).astype(jnp.bfloat16)
    padded = jnp.concatenate([normed, jnp.zeros((1, model_dim), jnp.bfloat16)], 0)
    expert_count = expert_gate.shape[0]
    flat_ids = route_ids.reshape(-1)
    pair_count = flat_ids.shape[0]
    per_block = TOK_MOE * TOP
    matches = (flat_ids[:, None] == jnp.arange(expert_count, dtype=jnp.int32)[None, :]).astype(jnp.int32)
    running = jnp.cumsum(matches.reshape(N_EP, per_block, expert_count), axis=1).reshape(pair_count, expert_count)
    slot_number = lax.optimization_barrier(jnp.sum((running - 1) * matches, axis=1)).astype(jnp.int32)
    source = (jnp.arange(pair_count, dtype=jnp.int32) // per_block).astype(jnp.int32)
    slot_index = (flat_ids * (N_EP * CAP) + source * CAP + slot_number).astype(jnp.int32)
    token_index = (jnp.arange(pair_count, dtype=jnp.int32) // TOP).astype(jnp.int32)
    slot_table = jnp.full((expert_count * N_EP * CAP,), token_count, jnp.int32).at[slot_index].set(token_index)

    def one_expert(pieces):
        table_rows, gate_weight, up_weight, down_weight = pieces
        inputs = padded[table_rows]
        gate_pre = jnp.dot(inputs, gate_weight, preferred_element_type=jnp.float32)
        up_pre = jnp.dot(inputs, up_weight, preferred_element_type=jnp.float32)
        hidden = (jax.nn.silu(gate_pre) * up_pre).astype(jnp.bfloat16)
        return jnp.dot(hidden, down_weight, preferred_element_type=jnp.float32).astype(jnp.bfloat16)
    results = lax.map(one_expert, (slot_table.reshape(expert_count, N_EP * CAP), expert_gate, expert_up, expert_down))
    picked = results.reshape(-1, model_dim)[slot_index].astype(jnp.float32).reshape(token_count, TOP, model_dim)
    combined = lax.optimization_barrier(jnp.sum(picked * route_weights[:, :, None], axis=1))
    return combined.astype(jnp.bfloat16)

def reference(query_in, key_in, value_in, gate_in, decay_rate, head_gain, output_weight, token_rows, token_gain, route_ids, route_weights, expert_gate, expert_up, expert_down):
    retained_out = retention(query_in, key_in, value_in, gate_in, decay_rate, head_gain, output_weight)
    expert_out = experts(token_rows, token_gain, route_ids, route_weights, expert_gate, expert_up, expert_down)
    return (retained_out, expert_out)
```

```python
import functools

import jax
import jax.numpy as jnp
import numpy as np
from jax import lax
from jax.experimental import pallas as pl
from jax.experimental.pallas import tpu as pltpu
from jax.sharding import PartitionSpec as P

epsilon = 1e-06
rope_base = 10000.0
UNITS = 8
SPLIT = (4, 5, 6)
GROUPS = ((0,), (1,), (2,), (3,), (4, 5), (6,), (7,))
F32 = jnp.float32
BF16 = jnp.bfloat16
MESH = pl.DeviceIdType.MESH


def dot(a, b):
    return jnp.dot(a, b, preferred_element_type=F32)


def iota(shape, dim):
    return lax.broadcasted_iota(jnp.int32, shape, dim)


def silu(v):
    return v / (1.0 + jnp.exp(-v))


def kernel(
    size,
    tgain, ids_t, rweights_t, decay, hgain, freq, turn_sign,
    tok_h, wg_h, wu_h, query_h, key_h, value_h, gate_h, ow_h, wd_h,
    ret_out, exp_out,
    tok, wg, wu, query, key, value, gate, ow, wd,
    normed, obuf, xbuf, hbuf, sbuf, rbuf, w_hi, w_lo, cos_t, sin_t,
    rq, rk, local, state, total_state, st_send, st_recv, mixed, part, rs1, rs2_send, rs2_recv,
    load_sem, d_send, d_recv, xy_send, xy_recv, xc_send, xc_recv,
    hy_send, hy_recv, hc_send, hc_recv, b_send, b_recv, st_ssem, st_rsem,
    r1_send, r1_recv, r2_send, r2_recv,
):
    ep, tp, cap, rounds, per, groups = (
        size["ep"], size["tp"], size["cap"], size["rounds"], size["per"], size["groups"]
    )
    ys = tp // 2
    e, t = lax.axis_index("ep"), lax.axis_index("tp")
    y, c = t // 2, lax.rem(t, 2)
    mate = (e, y * 2 + 1 - c)
    heads = decay.shape[0]
    tokens, model = tok.shape
    half = model // 2
    block_len = query.shape[0]
    dk = query.shape[1] // heads

    def bit(b):
        return lax.rem(e // 2**b, 2)

    def flipped(k):
        out = e
        for b in range(rounds):
            if k >> b & 1:
                out = out + (1 - 2 * bit(b)) * 2**b
        return out

    def pair(k):
        return (flipped(k), t)

    def y_at(offset):
        return lax.rem(y + offset, ys)

    def over_y(offset):
        return (e, y_at(offset) * 2 + c)

    def remote(src, dst, ssem, rsem, device):
        return pltpu.make_async_remote_copy(
            src_ref=src, dst_ref=dst, send_sem=ssem, recv_sem=rsem,
            device_id=device, device_id_type=MESH,
        )

    sent = []

    def send(src, dst, ssem, rsem, device):
        copy = remote(src, dst, ssem, rsem, device)
        copy.start()
        sent.append(copy)

    def arrived(dst, ssem, rsem, device):
        remote(dst, dst, ssem, rsem, device).wait_recv()

    loads = {
        name: pltpu.make_async_copy(a, b, load_sem.at[i])
        for i, (name, a, b) in enumerate((
            ("tok", tok_h, tok), ("wg", wg_h, wg), ("wu", wu_h, wu), ("query", query_h, query),
            ("key", key_h, key), ("value", value_h, value), ("gate", gate_h, gate),
            ("ow", ow_h, ow), ("wd", wd_h, wd)))
    }
    for copy in loads.values():
        copy.start()

    barrier = pltpu.get_barrier_semaphore()
    friends = [pair(k) for k in range(1, ep)] + [over_y(i) for i in range(1, ys)] + [mate]
    for friend in friends:
        pl.semaphore_signal(barrier, inc=1, device_id=friend, device_id_type=MESH)

    rows = max(ep, 16)
    after = jnp.where(
        iota((tokens, tokens), 0) < iota((tokens, tokens), 1), 1.0, 0.0).astype(BF16)

    def positions(ids):
        rel = jnp.bitwise_xor(ids, e)
        named = [iota((rows, tokens), 0) == rel[i:i + 1, :] for i in range(2)]
        rank = dot(jnp.where(named[0] | named[1], 1.0, 0.0).astype(BF16), after)
        return [
            rel[i:i + 1, :] * cap + jnp.sum(
                jnp.where(named[i], rank, 0.0), 0, keepdims=True).astype(jnp.int32)
            for i in range(2)
        ]

    def picks(pos, k, n):
        row_id = k * cap + iota((n * cap, tokens), 0)
        return jnp.where((row_id == pos[0]) | (row_id == pos[1]), 1.0, 0.0).astype(BF16)

    pos_t = positions(ids_t[...])
    loads["tok"].wait()
    rows_float = tok[...].astype(F32)
    scale = lax.rsqrt(jnp.mean(rows_float * rows_float, -1, keepdims=True) + epsilon)
    normed[...] = (rows_float * scale * tgain[...]).astype(BF16)

    def block(j, n=1):
        return pl.ds(j * cap, n * cap)

    def unit(u, n=1):
        return block(u * per, n * per)

    mine = pl.ds(pl.multiple_of(c * half, half), half)
    def blocks(u):
        return [k for k in range(u * per, (u + 1) * per) if k > 0]

    quarter = half // ys

    def part_cols(i):
        return pl.ds(pl.multiple_of(i * quarter, quarter), quarter)

    def push(u):
        if u in SPLIT:
            cols, source = part_cols(y), pl.ds(
                pl.multiple_of(c * half + y * quarter, quarter), quarter)
        else:
            cols, source = pl.ds(0, half), mine
        obuf[unit(u), cols] = dot(picks(pos_t, u * per, per), normed[:, source]).astype(BF16)
        for k in blocks(u):
            send(obuf.at[block(k), cols], xbuf.at[c, block(k), cols], d_send.at[k], d_recv.at[k],
                 pair(k))

    def landed(u, cols):
        for k in blocks(u):
            arrived(xbuf.at[c, block(k), cols], d_send.at[k], d_recv.at[k], pair(k))

    def y_relay(u):
        landed(u, part_cols(y))
        for a in range(1, ys):
            ref = xbuf.at[c, unit(u), part_cols(y)]
            send(ref, ref, xy_send.at[a, u], xy_recv.at[a, u], over_y(a))

    def x_relay(u):
        if not blocks(u):
            return
        if u in SPLIT:
            for a in range(1, ys):
                arrived(xbuf.at[c, unit(u), part_cols(y_at(ys - a))], xy_send.at[a, u],
                        xy_recv.at[a, u], over_y(a))
        else:
            landed(u, pl.ds(0, half))
        send(xbuf.at[c, unit(u)], xbuf.at[c, unit(u)], xc_send.at[u], xc_recv.at[u], mate)

    def own_block():
        if per == 1:
            own = picks(pos_t, 0, 1)
            for i in range(2):
                xbuf[i, block(0), :] = dot(own, normed[:, pl.ds(i * half, half)]).astype(BF16)
        else:
            xbuf[c, block(0), :] = obuf[block(0), :]

    pl.semaphore_wait(barrier, len(friends))
    def x_collect(u):
        if not blocks(u):
            return
        arrived(xbuf.at[1 - c, unit(u)], xc_send.at[u], xc_recv.at[u], mate)

    ff = wg.shape[1]
    n_tile = min(256, ff)

    def group_rows(g):
        return unit(groups[g][0], len(groups[g]))

    def up(g):
        for u in groups[g]:
            x_collect(u)
        rws = group_rows(g)

        def tile(n, carry):
            cols = pl.ds(pl.multiple_of(n * n_tile, n_tile), n_tile)
            a = v = None
            for p in range(2):
                x = xbuf[p, rws, :]
                ins = pl.ds(p * half, half)
                gp, vp = dot(x, wg[ins, cols]), dot(x, wu[ins, cols])
                a, v = (gp, vp) if a is None else (a + gp, v + vp)
            hbuf[t, rws, cols] = (silu(a) * v).astype(BF16)
            return carry

        lax.fori_loop(0, ff // n_tile, tile, 0)
        for a in range(1, ys):
            send(hbuf.at[t, rws], hbuf.at[t, rws], hy_send.at[a, g], hy_recv.at[a, g], over_y(a))
        send(hbuf.at[t, rws], hbuf.at[t, rws], hc_send.at[0, g], hc_recv.at[0, g], mate)

    def h_pass(g):
        rws = group_rows(g)
        for a in range(1, ys):
            piece = y_at(ys - a) * 2 + c
            arrived(hbuf.at[piece, rws], hy_send.at[a, g], hy_recv.at[a, g], over_y(a))
            send(hbuf.at[piece, rws], hbuf.at[piece, rws], hc_send.at[a, g], hc_recv.at[a, g],
                 mate)

    cw = wd.shape[1]
    d_tile = min(256, cw)

    def down(g):
        rws = group_rows(g)
        for a in range(ys):
            piece = y_at(ys - a) * 2 + 1 - c
            arrived(hbuf.at[piece, rws], hc_send.at[a, g], hc_recv.at[a, g], mate)

        def tile(n, carry):
            cols = pl.ds(pl.multiple_of(n * d_tile, d_tile), d_tile)
            total = None
            for p in range(tp):
                now = dot(hbuf[p, rws, :], wd[pl.ds(p * ff, ff), cols])
                total = now if total is None else total + now
            sbuf[rws, cols] = total.astype(BF16)
            return carry

        lax.fori_loop(0, cw // d_tile, tile, 0)
        for u in groups[g]:
            for k in range(u * per, (u + 1) * per):
                if k > 0:
                    send(sbuf.at[block(k)], rbuf.at[block(k)], b_send.at[k], b_recv.at[k], pair(k))
                else:
                    rbuf[block(0), :] = sbuf[block(0), :]

    within = iota((block_len, 1), 0).astype(F32)

    def head_cols(h):
        return pl.ds(pl.multiple_of(h * dk, dk), dk)

    def turn(x):
        return x * cos_t[...] + pltpu.roll(x, dk // 2, 1) * sin_t[...]

    def states():
        for name in ("query", "key", "value"):
            loads[name].wait()
        angles = (e * block_len + iota((block_len, dk), 0)).astype(F32) * freq[...]
        cos_t[...] = jnp.cos(angles)
        sin_t[...] = jnp.sin(angles) * turn_sign[...]

        def one(h, carry):
            cols = head_cols(h)
            rate = decay[h]
            rq[:, cols] = turn(query[:, cols].astype(F32)).astype(BF16)
            rot_key = (turn(key[:, cols].astype(F32)) * dk ** (-0.5)).astype(BF16)
            rk[:, cols] = rot_key
            decayed = (rot_key.astype(F32) * jnp.exp(-rate * (block_len - 1.0 - within))).astype(BF16)
            now = lax.dot_general(
                decayed, value[:, cols], (((0,), (0,)), ((), ())), preferred_element_type=F32)
            total_state[h] = now
            state[h] = jnp.zeros((dk, dk), F32)
            return carry

        lax.fori_loop(0, heads, one, 0)

    def lane(h, times):
        return jnp.exp(jnp.full((1, dk), -decay[h] * (block_len * times), F32))

    last = rounds - 1

    def state_copy(r):
        return remote(st_send.at[r], st_recv.at[r], st_ssem.at[r], st_rsem.at[r], pair(2**r))

    def state_send(r):
        def one(h, carry):
            st_send[r, h] = total_state[h].astype(BF16)
            return carry

        lax.fori_loop(0, heads, one, 0)
        if r < last:
            copy = state_copy(r)
            copy.start()
            sent.append(copy)
        else:
            @pl.when(bit(r) == 0)
            def _():
                state_copy(r).start()

    def state_take(r):
        later = bit(r) == 1
        before = lax.rem(e, 2**r).astype(F32)

        def one(h, carry):
            got = st_recv[r, h].astype(F32)
            state[h] = state[h] + jnp.where(later, got * lane(h, before), 0.0)
            if r < last:
                far = lane(h, float(2**r))
                total_state[h] = jnp.where(
                    later, got * far + total_state[h], total_state[h] * far + got)
            return carry

        def take():
            state_copy(r).wait_recv()
            lax.fori_loop(0, heads, one, 0)

        if r < last:
            take()
        else:
            pl.when(later)(take)

    def combine_weights():
        diagonal = iota((tokens, tokens), 0) == iota((tokens, tokens), 1)

        def upright(row):
            return jnp.sum(jnp.where(diagonal, row, 0.0), 1, keepdims=True)

        col = iota((tokens, ep * cap), 1)
        pos0 = upright(pos_t[0].astype(F32)).astype(jnp.int32)
        pos1 = upright(pos_t[1].astype(F32)).astype(jnp.int32)
        weight = jnp.where(col == pos0, upright(rweights_t[0:1, :]), 0.0) + jnp.where(
            col == pos1, upright(rweights_t[1:2, :]), 0.0)
        high = weight.astype(BF16)
        w_hi[...] = high
        w_lo[...] = (weight - high.astype(F32)).astype(BF16)

    chunk = min(128, block_len)

    def head_local(first, last):
        def step(n, carry):
            h, i = n // (block_len // chunk), lax.rem(n, block_len // chunk)
            cols = head_cols(h)
            rate = decay[h]
            key_grow = jnp.exp(rate * iota((1, block_len), 1).astype(F32))
            rws = pl.ds(pl.multiple_of(i * chunk, chunk), chunk)
            place = i * chunk + iota((chunk, 1), 0)
            scores = lax.dot_general(
                rq[rws, cols], rk[:, cols], (((1,), (1,)), ((), ())), preferred_element_type=F32)
            fade = jnp.exp(-rate * place.astype(F32)) * key_grow
            seen = iota((chunk, block_len), 1) <= place
            weights = jnp.where(seen, scores * fade, 0.0).astype(BF16)
            local[rws, cols] = dot(weights, value[:, cols])
            return carry

        n = block_len // chunk
        lax.fori_loop(first * n, last * n, step, 0)

    def finish():
        def step(n, carry):
            h, i = n // (block_len // chunk), lax.rem(n, block_len // chunk)
            cols = head_cols(h)
            rws = pl.ds(pl.multiple_of(i * chunk, chunk), chunk)
            place = (i * chunk + iota((chunk, 1), 0)).astype(F32)
            held = state[h]
            high = held.astype(BF16)
            low = (held - high.astype(F32)).astype(BF16)
            q = rq[rws, cols]
            retained = local[rws, cols] + (dot(q, high) + dot(q, low)) * jnp.exp(
                -decay[h] * (place + 1.0))
            centered = retained - jnp.mean(retained, -1, keepdims=True)
            out = centered * lax.rsqrt(jnp.mean(centered * centered, -1, keepdims=True) + epsilon)
            mixed[rws, cols] = (
                out * hgain[:, cols] * silu(gate[rws, cols].astype(F32))).astype(BF16)
            return carry

        lax.fori_loop(0, heads * (block_len // chunk), step, 0)

    rb = block_len // tp
    o_tile = min(512, model)

    def project():
        def step(n, carry):
            cols = pl.ds(pl.multiple_of(n * o_tile, o_tile), o_tile)
            for d in range(tp):
                part[d, :, cols] = dot(mixed[pl.ds(d * rb, rb), :], ow[:, cols]).astype(BF16)
            return carry

        lax.fori_loop(0, model // o_tile, step, 0)
        for b in range(ys):
            send(part.at[b * 2 + 1 - c], rs1.at[b], r1_send.at[b], r1_recv.at[b], mate)

    def sum_over_cores():
        for b in range(ys):
            arrived(rs1.at[b], r1_send.at[b], r1_recv.at[b], mate)
        for a in range(1, ys):
            b = y_at(a)
            rs2_send[a - 1] = (part[b * 2 + c].astype(F32) + rs1[b].astype(F32)).astype(BF16)
            send(rs2_send.at[a - 1], rs2_recv.at[a - 1], r2_send.at[a - 1], r2_recv.at[a - 1],
                 over_y(a))

    if blocks(0):
        push(0)
    push(1)
    push(2)
    push(3)
    own_block()
    loads["wg"].wait()
    loads["wu"].wait()
    x_relay(0)
    up(0)
    states()
    state_send(0)
    push(4)
    push(5)
    x_relay(1)
    up(1)
    x_relay(2)
    h_pass(0)
    up(2)
    y_relay(4)
    x_relay(3)
    state_take(0)
    state_send(1)
    push(6)
    y_relay(5)
    up(3)
    h_pass(1)
    state_take(1)
    state_send(2)
    push(7)
    head_local(0, heads)
    h_pass(2)
    x_relay(4)
    x_relay(5)
    combine_weights()
    for r in range(3, rounds):
        state_take(r - 1)
        state_send(r)
    y_relay(6)
    up(4)
    h_pass(3)
    state_take(last)
    loads["gate"].wait()
    loads["ow"].wait()
    finish()
    x_relay(6)
    project()
    up(5)
    loads["wd"].wait()
    x_relay(7)
    h_pass(4)
    up(6)
    down(4)
    sum_over_cores()
    down(0)
    down(1)
    h_pass(5)
    down(2)
    down(3)
    down(5)
    h_pass(6)
    down(6)

    total = part[t].astype(F32) + rs1[y].astype(F32)
    for a in range(1, ys):
        arrived(rs2_recv.at[a - 1], r2_send.at[a - 1], r2_recv.at[a - 1], over_y(a))
        total += rs2_recv[a - 1].astype(F32)
    ret_out[...] = total.astype(BF16)
    for k in range(1, ep):
        arrived(rbuf.at[block(k)], b_send.at[k], b_recv.at[k], pair(k))
    exp_out[...] = (dot(w_hi[...], rbuf[...]) + dot(w_lo[...], rbuf[...])).astype(BF16)
    for copy in sent:
        copy.wait_send()

    @pl.when(bit(last) == 0)
    def _():
        state_copy(last).wait_send()


def body(
    query_in, key_in, value_in, gate_in, decay_rate, head_gain, output_weight,
    token_rows, token_gain, route_ids, route_weights, expert_gate, expert_up, expert_down,
):
    ep, tp = lax.axis_size("ep"), lax.axis_size("tp")
    tokens, model = token_rows.shape
    top = route_ids.shape[1]
    cap = -(-(2 * tokens * top // ep) // 32) * 32
    block_len, width = query_in.shape
    heads = decay_rate.shape[0]
    dk = width // heads
    ff = expert_gate.shape[2]
    cw = expert_down.shape[2]
    ys = tp // 2
    rounds = ep.bit_length() - 1
    assert ep == 2**rounds and rounds >= 3
    per = ep // UNITS
    turns = dk // 2
    freq = np.tile(
        np.float32(rope_base) ** (-np.arange(turns, dtype=np.float32) * np.float32(2.0 / dk)), 2)
    turn_sign = np.where(np.arange(dk) < turns, -1.0, 1.0)
    size = dict(ep=ep, tp=tp, cap=cap, rounds=rounds, per=per, groups=GROUPS)
    slots = ep * cap
    rb = block_len // tp
    vmem = pl.BlockSpec(memory_space=pltpu.VMEM)
    smem = pl.BlockSpec(memory_space=pltpu.SMEM)
    hbm = pl.BlockSpec(memory_space=pl.ANY)
    dma = pltpu.SemaphoreType.DMA
    big = [token_rows, expert_gate[0], expert_up[0], query_in, key_in, value_in, gate_in,
           output_weight, expert_down[0]]
    nm = len(GROUPS)
    return pl.pallas_call(
        functools.partial(kernel, size),
        out_shape=(
            jax.ShapeDtypeStruct((rb, model), BF16),
            jax.ShapeDtypeStruct((tokens, cw), BF16),
        ),
        in_specs=[vmem] * 3 + [smem] + [vmem] * 3 + [hbm] * 9,
        out_specs=(vmem, vmem),
        scratch_shapes=[pltpu.VMEM(a.shape, BF16) for a in big]
        + [
            pltpu.VMEM((tokens, model), BF16),
            pltpu.VMEM((slots, model // 2), BF16),
            pltpu.VMEM((2, slots, model // 2), BF16),
            pltpu.VMEM((tp, slots, ff), BF16),
            pltpu.VMEM((slots, cw), BF16),
            pltpu.VMEM((slots, cw), BF16),
            pltpu.VMEM((tokens, slots), BF16),
            pltpu.VMEM((tokens, slots), BF16),
            pltpu.VMEM((block_len, dk), F32),
            pltpu.VMEM((block_len, dk), F32),
            pltpu.VMEM((block_len, width), BF16),
            pltpu.VMEM((block_len, width), BF16),
            pltpu.VMEM((block_len, width), F32),
            pltpu.VMEM((heads, dk, dk), F32),
            pltpu.VMEM((heads, dk, dk), F32),
            pltpu.VMEM((rounds, heads, dk, dk), BF16),
            pltpu.VMEM((rounds, heads, dk, dk), BF16),
            pltpu.VMEM((block_len, width), BF16),
            pltpu.VMEM((tp, rb, model), BF16),
            pltpu.VMEM((ys, rb, model), BF16),
            pltpu.VMEM((max(ys - 1, 1), rb, model), BF16),
            pltpu.VMEM((max(ys - 1, 1), rb, model), BF16),
            dma((9,)),
            dma((ep,)), dma((ep,)),
            dma((ys, UNITS)), dma((ys, UNITS)), dma((UNITS,)), dma((UNITS,)),
            dma((ys, nm)), dma((ys, nm)), dma((ys, nm)), dma((ys, nm)),
            dma((ep,)), dma((ep,)),
            dma((rounds,)), dma((rounds,)),
            dma((ys,)), dma((ys,)), dma((ys,)), dma((ys,)),
        ],
        compiler_params=pltpu.CompilerParams(
            collective_id=0, has_side_effects=True, vmem_limit_bytes=60 * 2**20
        ),
    )(
        token_gain[None, :], route_ids.T, route_weights.T,
        decay_rate, head_gain[None, :],
        jnp.asarray(freq[None, :], F32), jnp.asarray(turn_sign[None, :], F32),
        *big,
    )


def solution(mesh):
    placed = (
        P("ep", "tp"), P("ep", "tp"), P("ep", "tp"), P("ep", "tp"),
        P("tp"), P("tp"), P("tp", None), P("ep", None), P(),
        P("ep", None), P("ep", None),
        P("ep", None, "tp"), P("ep", None, "tp"), P("ep", None, "tp"),
    )
    return jax.shard_map(
        body,
        mesh=mesh,
        in_specs=placed,
        out_specs=(P(("ep", "tp"), None), P("ep", "tp")),
        check_vma=False,
    )
```

```python
import functools

import jax
import jax.numpy as jnp
import numpy as np
from jax import lax
from jax.experimental import pallas as pl
from jax.experimental.pallas import tpu as pltpu
from jax.sharding import PartitionSpec as P

epsilon = 1e-06
rope_base = 10000.0
UNITS, PIECES = 8, 2
GROUPS = tuple((u,) for u in range(UNITS))
F32 = jnp.float32
BF16 = jnp.bfloat16
MESH = pl.DeviceIdType.MESH


def dot(a, b):
    return jnp.dot(a, b, preferred_element_type=F32)


def iota(shape, dim):
    return lax.broadcasted_iota(jnp.int32, shape, dim)


def silu(v):
    return v / (1.0 + jnp.exp(-v))


def kernel(
    size,
    ids_h, tok_h, tgain_h, wg_h, wu_h, query_h, key_h, value_h, decay_h, freq_h, sign_h,
    rweights_h, gate_h, hgain_h, ow_h, wd_h,
    ret_out, exp_out,
    ids_t, tok, tgain, wg, wu, query, key, value, decay, freq, turn_sign,
    rweights_t, gate, hgain, ow, wd,
    normed, raw, ids_in, far_picks, obuf, xbuf, hbuf, gate_acc, up_acc, sbuf, rbuf, w_hi, w_lo, cos_t, sin_t,
    rq, rk, local, state, total_state, st_send, st_recv, mixed, part, rs1, rs2_send, rs2_recv,
    load_sem, id_send, id_recv, raw_send, raw_recv, ry_send, ry_recv, d_send, d_recv, xc_send, xc_recv,
    hy_send, hy_recv, hc_send, hc_recv, b_send, b_recv, st_ssem, st_rsem,
    r1_send, r1_recv, r2_send, r2_recv, ret, exp, out_sem,
):
    ep, tp, cap, rounds, per, groups = (
        size["ep"], size["tp"], size["cap"], size["rounds"], size["per"], size["groups"]
    )
    ys = tp // 2
    e, t = lax.axis_index("ep"), lax.axis_index("tp")
    y, c = t // 2, lax.rem(t, 2)
    mate = (e, y * 2 + 1 - c)
    heads = decay.shape[0]
    tokens, model = tok.shape
    half = model // 2
    block_len = query.shape[0]
    dk = query.shape[1] // heads

    def bit(b):
        return lax.rem(e // 2**b, 2)

    def flipped(k):
        out = e
        for b in range(rounds):
            if k >> b & 1:
                out = out + (1 - 2 * bit(b)) * 2**b
        return out

    def pair(k):
        return (flipped(k), t)

    def y_at(offset):
        return lax.rem(y + offset, ys)

    def over_y(offset):
        return (e, y_at(offset) * 2 + c)

    def remote(src, dst, ssem, rsem, device):
        return pltpu.make_async_remote_copy(
            src_ref=src, dst_ref=dst, send_sem=ssem, recv_sem=rsem,
            device_id=device, device_id_type=MESH,
        )

    sent = []

    def send(src, dst, ssem, rsem, device):
        copy = remote(src, dst, ssem, rsem, device)
        copy.start()
        sent.append(copy)

    def arrived(dst, ssem, rsem, device):
        remote(dst, dst, ssem, rsem, device).wait_recv()

    loads = {
        name: pltpu.make_async_copy(a, b, load_sem.at[i])
        for i, (name, a, b) in enumerate((
            ("ids", ids_h, ids_t), ("tok", tok_h, tok), ("tgain", tgain_h, tgain),
            ("wg", wg_h, wg), ("wu", wu_h, wu), ("query", query_h, query), ("key", key_h, key),
            ("value", value_h, value), ("decay", decay_h, decay), ("freq", freq_h, freq),
            ("sign", sign_h, turn_sign), ("rweights", rweights_h, rweights_t),
            ("gate", gate_h, gate), ("hgain", hgain_h, hgain), ("ow", ow_h, ow), ("wd", wd_h, wd)))
    }
    for copy in loads.values():
        copy.start()

    barrier = pltpu.get_barrier_semaphore()
    friends = [pair(k) for k in range(1, ep)] + [over_y(i) for i in range(1, ys)] + [mate]
    for friend in friends:
        pl.semaphore_signal(barrier, inc=1, device_id=friend, device_id_type=MESH)

    rows = max(ep, 16)
    after = jnp.where(
        iota((tokens, tokens), 0) < iota((tokens, tokens), 1), 1.0, 0.0).astype(BF16)

    def positions(ids):
        rel = jnp.bitwise_xor(ids, e)
        named = [iota((rows, tokens), 0) == rel[i:i + 1, :] for i in range(2)]
        rank = dot(jnp.where(named[0] | named[1], 1.0, 0.0).astype(BF16), after)
        return [
            rel[i:i + 1, :] * cap + jnp.sum(
                jnp.where(named[i], rank, 0.0), 0, keepdims=True).astype(jnp.int32)
            for i in range(2)
        ]

    def picks(pos, k, n):
        row_id = k * cap + iota((n * cap, tokens), 0)
        return jnp.where((row_id == pos[0]) | (row_id == pos[1]), 1.0, 0.0).astype(BF16)

    loads["ids"].wait()
    pos_t = positions(ids_t[...])
    loads["tok"].wait()
    loads["tgain"].wait()
    rows_float = tok[...].astype(F32)
    scale = lax.rsqrt(jnp.mean(rows_float * rows_float, -1, keepdims=True) + epsilon)
    normed[...] = (rows_float * scale * tgain[...]).astype(BF16)

    def block(j, n=1):
        return pl.ds(j * cap, n * cap)

    def unit(u, n=1):
        return block(u * per, n * per)

    mine = pl.ds(pl.multiple_of(c * half, half), half)
    def blocks(u):
        return [k for k in range(u * per, (u + 1) * per) if k > 0]

    units = ep // per
    far, near = ep // 2, units // 2
    pieces = size["pieces"]
    width = half // pieces
    strip = width // ys

    def piece(i):
        return pl.ds(i * width, width)

    def strip_cols(i, at):
        return pl.ds(pl.multiple_of(i * width + at * strip, strip), strip)

    def push(u):
        obuf[unit(u), :] = dot(picks(pos_t, u * per, per), normed[:, mine]).astype(BF16)
        for k in blocks(u):
            send(obuf.at[block(k)], xbuf.at[c, block(k)], d_send.at[k, 0], d_recv.at[k, 0],
                 pair(k))

    def raw_push(i):
        if i == 0:
            send(ids_t, ids_in, id_send.at[0], id_recv.at[0], pair(far))
        cols = pl.ds(pl.multiple_of(c * half + i * width + y * strip, strip), strip)
        send(normed.at[:, cols], raw.at[:, strip_cols(i, y)], raw_send.at[i], raw_recv.at[i],
             pair(far))

    def raw_relay(i):
        ref = raw.at[:, strip_cols(i, y)]
        arrived(ref, raw_send.at[i], raw_recv.at[i], pair(far))
        for a in range(1, ys):
            send(ref, ref, ry_send.at[a, i], ry_recv.at[a, i], over_y(a))

    def far_select(i):
        if i == 0:
            arrived(ids_in, id_send.at[0], id_recv.at[0], pair(far))
            far_picks[...] = picks(positions(ids_in[...]), 0, far)
        for a in range(1, ys):
            arrived(raw.at[:, strip_cols(i, y_at(ys - a))], ry_send.at[a, i], ry_recv.at[a, i],
                    over_y(a))
        for u in range(near):
            chosen = dot(far_picks[unit(u), :], raw[:, piece(i)]).astype(BF16)
            obuf[unit(near + u), piece(i)] = chosen
            if u == 0:
                xbuf[c, block(far), piece(i)] = chosen[:cap]
            for k in blocks(u):
                j = far + k
                send(obuf.at[block(j), piece(i)], xbuf.at[c, block(j), piece(i)],
                     d_send.at[j, i], d_recv.at[j, i], pair(k))

    def landed(u):
        for k in blocks(u):
            if k < far:
                arrived(xbuf.at[c, block(k)], d_send.at[k, 0], d_recv.at[k, 0], pair(k))
            elif k > far:
                for i in range(pieces):
                    arrived(xbuf.at[c, block(k), piece(i)], d_send.at[k, i], d_recv.at[k, i],
                            pair(k - far))

    def x_relay(u):
        if not blocks(u):
            return
        landed(u)
        send(xbuf.at[c, unit(u)], xbuf.at[c, unit(u)], xc_send.at[u], xc_recv.at[u], mate)

    def own_block():
        if per == 1:
            own = picks(pos_t, 0, 1)
            for i in range(2):
                xbuf[i, block(0), :] = dot(own, normed[:, pl.ds(i * half, half)]).astype(BF16)
        else:
            xbuf[c, block(0), :] = obuf[block(0), :]

    pl.semaphore_wait(barrier, len(friends))
    def x_collect(u):
        if not blocks(u):
            return
        arrived(xbuf.at[1 - c, unit(u)], xc_send.at[u], xc_recv.at[u], mate)

    ff = wg.shape[1]
    n_tile = min(256, ff)

    def group_rows(g):
        return unit(groups[g][0], len(groups[g]))

    def up(g):
        for u in groups[g]:
            x_collect(u)
        rws = group_rows(g)

        def tile(n, carry):
            cols = pl.ds(pl.multiple_of(n * n_tile, n_tile), n_tile)
            a = v = None
            for p in range(2):
                x = xbuf[p, rws, :]
                ins = pl.ds(p * half, half)
                gp, vp = dot(x, wg[ins, cols]), dot(x, wu[ins, cols])
                a, v = (gp, vp) if a is None else (a + gp, v + vp)
            hbuf[t, rws, cols] = (silu(a) * v).astype(BF16)
            return carry

        lax.fori_loop(0, ff // n_tile, tile, 0)

    def up_half(g, core):
        ins = pl.ds(pl.multiple_of(core * half, half), half)
        rws = group_rows(g)

        def products(n):
            cols = pl.ds(pl.multiple_of(n * n_tile, n_tile), n_tile)
            x = xbuf[core, rws, :]
            return cols, dot(x, wg[ins, cols]), dot(x, wu[ins, cols])

        return rws, products

    def up_mine(g):
        rws, products = up_half(g, c)

        def tile(n, carry):
            cols, a, v = products(n)
            gate_acc[:, cols] = a
            up_acc[:, cols] = v
            return carry

        lax.fori_loop(0, ff // n_tile, tile, 0)

    def up_rest(g):
        for u in groups[g]:
            x_collect(u)
        rws, products = up_half(g, 1 - c)

        def tile(n, carry):
            cols, a, v = products(n)
            hbuf[t, rws, cols] = (silu(gate_acc[:, cols] + a) * (up_acc[:, cols] + v)).astype(BF16)
            return carry

        lax.fori_loop(0, ff // n_tile, tile, 0)

    def up_send(g):
        rws = group_rows(g)
        for a in range(1, ys):
            send(hbuf.at[t, rws], hbuf.at[t, rws], hy_send.at[a, g], hy_recv.at[a, g], over_y(a))
        send(hbuf.at[t, rws], hbuf.at[t, rws], hc_send.at[0, g], hc_recv.at[0, g], mate)

    def h_pass(g):
        rws = group_rows(g)
        for a in range(1, ys):
            piece = y_at(ys - a) * 2 + c
            arrived(hbuf.at[piece, rws], hy_send.at[a, g], hy_recv.at[a, g], over_y(a))
            send(hbuf.at[piece, rws], hbuf.at[piece, rws], hc_send.at[a, g], hc_recv.at[a, g],
                 mate)

    cw = wd.shape[1]
    d_tile = min(256, cw)

    def down(g):
        rws = group_rows(g)
        for a in range(ys):
            piece = y_at(ys - a) * 2 + 1 - c
            arrived(hbuf.at[piece, rws], hc_send.at[a, g], hc_recv.at[a, g], mate)

        def tile(n, carry):
            cols = pl.ds(pl.multiple_of(n * d_tile, d_tile), d_tile)
            total = None
            for p in range(tp):
                now = dot(hbuf[p, rws, :], wd[pl.ds(p * ff, ff), cols])
                total = now if total is None else total + now
            sbuf[rws, cols] = total.astype(BF16)
            return carry

        lax.fori_loop(0, cw // d_tile, tile, 0)
        for u in groups[g]:
            for k in range(u * per, (u + 1) * per):
                if k > 0:
                    send(sbuf.at[block(k)], rbuf.at[block(k)], b_send.at[k], b_recv.at[k], pair(k))
                else:
                    rbuf[block(0), :] = sbuf[block(0), :]

    within = iota((block_len, 1), 0).astype(F32)

    def head_cols(h):
        return pl.ds(pl.multiple_of(h * dk, dk), dk)

    def turn(x):
        return x * cos_t[...] + pltpu.roll(x, dk // 2, 1) * sin_t[...]

    def states():
        for name in ("query", "key", "value", "decay", "freq", "sign"):
            loads[name].wait()
        angles = (e * block_len + iota((block_len, dk), 0)).astype(F32) * freq[...]
        cos_t[...] = jnp.cos(angles)
        sin_t[...] = jnp.sin(angles) * turn_sign[...]

        def one(h, carry):
            cols = head_cols(h)
            rate = decay[h]
            rq[:, cols] = turn(query[:, cols].astype(F32)).astype(BF16)
            rot_key = (turn(key[:, cols].astype(F32)) * dk ** (-0.5)).astype(BF16)
            rk[:, cols] = rot_key
            decayed = (rot_key.astype(F32) * jnp.exp(-rate * (block_len - 1.0 - within))).astype(BF16)
            now = lax.dot_general(
                decayed, value[:, cols], (((0,), (0,)), ((), ())), preferred_element_type=F32)
            total_state[h] = now
            state[h] = jnp.zeros((dk, dk), F32)
            return carry

        lax.fori_loop(0, heads, one, 0)

    def lane(h, times):
        return jnp.exp(jnp.full((1, dk), -decay[h] * (block_len * times), F32))

    last = rounds - 1

    def state_copy(r):
        return remote(st_send.at[r], st_recv.at[r], st_ssem.at[r], st_rsem.at[r], pair(2**r))

    def state_send(r):
        def one(h, carry):
            st_send[r, h] = total_state[h].astype(BF16)
            return carry

        lax.fori_loop(0, heads, one, 0)
        if r < last:
            copy = state_copy(r)
            copy.start()
            sent.append(copy)
        else:
            @pl.when(bit(r) == 0)
            def _():
                state_copy(r).start()

    def state_take(r):
        later = bit(r) == 1
        before = lax.rem(e, 2**r).astype(F32)

        def one(h, carry):
            got = st_recv[r, h].astype(F32)
            state[h] = state[h] + jnp.where(later, got * lane(h, before), 0.0)
            if r < last:
                far = lane(h, float(2**r))
                total_state[h] = jnp.where(
                    later, got * far + total_state[h], total_state[h] * far + got)
            return carry

        def take():
            state_copy(r).wait_recv()
            lax.fori_loop(0, heads, one, 0)

        if r < last:
            take()
        else:
            pl.when(later)(take)

    def combine_weights():
        diagonal = iota((tokens, tokens), 0) == iota((tokens, tokens), 1)

        def upright(row):
            return jnp.sum(jnp.where(diagonal, row, 0.0), 1, keepdims=True)

        col = iota((tokens, ep * cap), 1)
        pos0 = upright(pos_t[0].astype(F32)).astype(jnp.int32)
        pos1 = upright(pos_t[1].astype(F32)).astype(jnp.int32)
        weight = jnp.where(col == pos0, upright(rweights_t[0:1, :]), 0.0) + jnp.where(
            col == pos1, upright(rweights_t[1:2, :]), 0.0)
        high = weight.astype(BF16)
        w_hi[...] = high
        w_lo[...] = (weight - high.astype(F32)).astype(BF16)

    chunk = min(128, block_len)

    chunks = block_len // chunk

    def head_local(first, stop):
        def one(h, carry):
            cols = head_cols(h)
            rate = decay[h]
            key_grow = jnp.exp(rate * iota((1, block_len), 1).astype(F32))
            for i in range(chunks):
                seen_keys = (i + 1) * chunk
                rws, keys = pl.ds(i * chunk, chunk), pl.ds(0, seen_keys)
                place = i * chunk + iota((chunk, 1), 0)
                scores = lax.dot_general(
                    rq[rws, cols], rk[keys, cols], (((1,), (1,)), ((), ())),
                    preferred_element_type=F32)
                fade = jnp.exp(-rate * place.astype(F32)) * key_grow[:, :seen_keys]
                seen = iota((chunk, seen_keys), 1) <= place
                weights = jnp.where(seen, scores * fade, 0.0).astype(BF16)
                local[rws, cols] = dot(weights, value[keys, cols])
            return carry

        lax.fori_loop(first, stop, one, 0)

    def finish(first, stop):
        def one(h, carry):
            cols = head_cols(h)
            held = state[h]
            high = held.astype(BF16)
            low = (held - high.astype(F32)).astype(BF16)
            for i in range(chunks):
                rws = pl.ds(i * chunk, chunk)
                place = (i * chunk + iota((chunk, 1), 0)).astype(F32)
                q = rq[rws, cols]
                retained = local[rws, cols] + (dot(q, high) + dot(q, low)) * jnp.exp(
                    -decay[h] * (place + 1.0))
                centered = retained - jnp.mean(retained, -1, keepdims=True)
                out = centered * lax.rsqrt(
                    jnp.mean(centered * centered, -1, keepdims=True) + epsilon)
                mixed[rws, cols] = (
                    out * hgain[:, cols] * silu(gate[rws, cols].astype(F32))).astype(BF16)
            return carry

        lax.fori_loop(first, stop, one, 0)

    rb = block_len // tp
    o_tile = min(512, model)

    def project():
        def step(n, carry):
            cols = pl.ds(pl.multiple_of(n * o_tile, o_tile), o_tile)
            for d in range(tp):
                part[d, :, cols] = dot(mixed[pl.ds(d * rb, rb), :], ow[:, cols]).astype(BF16)
            return carry

        lax.fori_loop(0, model // o_tile, step, 0)
        for b in range(ys):
            send(part.at[b * 2 + 1 - c], rs1.at[b], r1_send.at[b], r1_recv.at[b], mate)

    def sum_over_cores():
        for b in range(ys):
            arrived(rs1.at[b], r1_send.at[b], r1_recv.at[b], mate)
        for a in range(1, ys):
            b = y_at(a)
            rs2_send[a - 1] = (part[b * 2 + c].astype(F32) + rs1[b].astype(F32)).astype(BF16)
            send(rs2_send.at[a - 1], rs2_recv.at[a - 1], r2_send.at[a - 1], r2_recv.at[a - 1],
                 over_y(a))

    if blocks(0):
        push(0)
    for u in range(1, near):
        push(u)
    own_block()
    loads["wg"].wait()
    loads["wu"].wait()
    x_relay(0)
    up(0)
    up_send(0)
    states()
    for i in range(pieces):
        raw_push(i)
    state_send(0)
    x_relay(1)
    up_mine(1)
    x_relay(2)
    up_rest(1)
    up_send(1)
    h_pass(0)
    head_local(0, heads)
    raw_relay(0)
    up(2)
    for i in range(1, pieces):
        raw_relay(i)
    up_send(2)
    state_take(0)
    state_send(1)
    x_relay(3)
    h_pass(1)
    far_select(0)
    up(3)
    up_send(3)
    loads["wd"].wait()
    down(0)
    for i in range(1, pieces):
        far_select(i)
    x_relay(4)
    up_mine(4)
    state_take(1)
    state_send(2)
    h_pass(2)
    up_rest(4)
    up_send(4)
    x_relay(5)
    x_relay(6)
    h_pass(3)
    down(1)
    up(5)
    up_send(5)
    for r in range(3, rounds):
        state_take(r - 1)
        state_send(r)
    x_relay(7)
    state_take(last)
    loads["gate"].wait()
    loads["hgain"].wait()
    loads["ow"].wait()
    finish(0, heads)
    h_pass(4)
    up(6)
    up_send(6)
    project()
    up(7)
    up_send(7)
    early = len(sent)
    h_pass(5)
    sum_over_cores()
    down(4)
    down(5)
    h_pass(6)
    down(2)
    down(6)
    down(3)
    loads["rweights"].wait()
    combine_weights()
    h_pass(7)
    down(7)

    for copy in sent[:early]:
        copy.wait_send()
    split = ep // 2
    for k in range(1, split):
        arrived(rbuf.at[block(k)], b_send.at[k], b_recv.at[k], pair(k))

    def weighed(cols):
        rows_back = rbuf[cols, :]
        return dot(w_hi[:, cols], rows_back) + dot(w_lo[:, cols], rows_back)

    close = weighed(block(0, split))
    total = part[t].astype(F32) + rs1[y].astype(F32)
    for a in range(1, ys):
        arrived(rs2_recv.at[a - 1], r2_send.at[a - 1], r2_recv.at[a - 1], over_y(a))
        total += rs2_recv[a - 1].astype(F32)
    ret[...] = total.astype(BF16)
    ret_store = pltpu.make_async_copy(ret, ret_out, out_sem.at[0])
    ret_store.start()
    for k in range(split, ep):
        arrived(rbuf.at[block(k)], b_send.at[k], b_recv.at[k], pair(k))
    exp[...] = (close + weighed(block(split, ep - split))).astype(BF16)
    exp_store = pltpu.make_async_copy(exp, exp_out, out_sem.at[1])
    exp_store.start()
    for copy in sent[early:]:
        copy.wait_send()
    ret_store.wait()
    exp_store.wait()

    @pl.when(bit(last) == 0)
    def _():
        state_copy(last).wait_send()


def hand_on(ret_in, exp_in, ret_out, exp_out, ret, exp, in_sem, out_sem):
    ways = ((ret_in, ret, ret_out), (exp_in, exp, exp_out))
    taken = [pltpu.make_async_copy(a, b, in_sem.at[i]) for i, (a, b, _) in enumerate(ways)]
    given = [pltpu.make_async_copy(b, d, out_sem.at[i]) for i, (_, b, d) in enumerate(ways)]
    for copy in taken:
        copy.start()
    for i in range(2):
        taken[i].wait()
        given[i].start()
    for copy in given:
        copy.wait()


def body(
    query_in, key_in, value_in, gate_in, decay_rate, head_gain, output_weight,
    token_rows, token_gain, route_ids, route_weights, expert_gate, expert_up, expert_down,
):
    ep, tp = lax.axis_size("ep"), lax.axis_size("tp")
    tokens, model = token_rows.shape
    top = route_ids.shape[1]
    cap = -(-(2 * tokens * top // ep) // 32) * 32
    block_len, width = query_in.shape
    heads = decay_rate.shape[0]
    dk = width // heads
    ff = expert_gate.shape[2]
    cw = expert_down.shape[2]
    ys = tp // 2
    rounds = ep.bit_length() - 1
    assert ep == 2**rounds and rounds >= 3
    per = ep // UNITS
    pieces = max(1, min(PIECES, model // (2 * 128 * ys)))
    turns = dk // 2
    freq = np.tile(
        np.float32(rope_base) ** (-np.arange(turns, dtype=np.float32) * np.float32(2.0 / dk)), 2)
    turn_sign = np.where(np.arange(dk) < turns, -1.0, 1.0)
    size = dict(ep=ep, tp=tp, cap=cap, rounds=rounds, per=per, groups=GROUPS, pieces=pieces)
    slots = ep * cap
    rb = block_len // tp
    hbm = pl.BlockSpec(memory_space=pl.ANY)
    dma = pltpu.SemaphoreType.DMA
    given = [
        route_ids.T, token_rows, token_gain[None, :], expert_gate[0], expert_up[0],
        query_in, key_in, value_in, decay_rate,
        jnp.asarray(freq[None, :], F32), jnp.asarray(turn_sign[None, :], F32),
        route_weights.T, gate_in, head_gain[None, :], output_weight, expert_down[0],
    ]
    nm = len(GROUPS)
    outs = pl.pallas_call(
        functools.partial(kernel, size),
        out_shape=(
            jax.ShapeDtypeStruct((rb, model), BF16),
            jax.ShapeDtypeStruct((tokens, cw), BF16),
        ),
        in_specs=[hbm] * len(given),
        out_specs=(hbm, hbm),
        scratch_shapes=[
            (pltpu.SMEM if a is decay_rate else pltpu.VMEM)(a.shape, a.dtype) for a in given]
        + [
            pltpu.VMEM((tokens, model), BF16),
            pltpu.VMEM((tokens, model // 2), BF16),
            pltpu.VMEM((top, tokens), jnp.int32),
            pltpu.VMEM((slots // 2, tokens), BF16),
            pltpu.VMEM((slots, model // 2), BF16),
            pltpu.VMEM((2, slots, model // 2), BF16),
            pltpu.VMEM((tp, slots, ff), BF16),
            pltpu.VMEM((per * cap, ff), F32),
            pltpu.VMEM((per * cap, ff), F32),
            pltpu.VMEM((slots, cw), BF16),
            pltpu.VMEM((slots, cw), BF16),
            pltpu.VMEM((tokens, slots), BF16),
            pltpu.VMEM((tokens, slots), BF16),
            pltpu.VMEM((block_len, dk), F32),
            pltpu.VMEM((block_len, dk), F32),
            pltpu.VMEM((block_len, width), BF16),
            pltpu.VMEM((block_len, width), BF16),
            pltpu.VMEM((block_len, width), F32),
            pltpu.VMEM((heads, dk, dk), F32),
            pltpu.VMEM((heads, dk, dk), F32),
            pltpu.VMEM((rounds, heads, dk, dk), BF16),
            pltpu.VMEM((rounds, heads, dk, dk), BF16),
            pltpu.VMEM((block_len, width), BF16),
            pltpu.VMEM((tp, rb, model), BF16),
            pltpu.VMEM((ys, rb, model), BF16),
            pltpu.VMEM((max(ys - 1, 1), rb, model), BF16),
            pltpu.VMEM((max(ys - 1, 1), rb, model), BF16),
            dma((len(given),)),
            dma((1,)), dma((1,)), dma((pieces,)), dma((pieces,)),
            dma((ys, pieces)), dma((ys, pieces)),
            dma((ep, pieces)), dma((ep, pieces)),
            dma((UNITS,)), dma((UNITS,)),
            dma((ys, nm)), dma((ys, nm)), dma((ys, nm)), dma((ys, nm)),
            dma((ep,)), dma((ep,)),
            dma((rounds,)), dma((rounds,)),
            dma((ys,)), dma((ys,)), dma((ys,)), dma((ys,)),
            pltpu.VMEM((rb, model), BF16),
            pltpu.VMEM((tokens, cw), BF16),
            dma((2,)),
        ],
        compiler_params=pltpu.CompilerParams(
            collective_id=0, has_side_effects=True, vmem_limit_bytes=60 * 2**20
        ),
    )(*given)
    return pl.pallas_call(
        hand_on,
        out_shape=tuple(jax.ShapeDtypeStruct(a.shape, a.dtype) for a in outs),
        in_specs=[hbm] * 2,
        out_specs=(hbm, hbm),
        scratch_shapes=[pltpu.VMEM(a.shape, a.dtype) for a in outs] + [dma((2,)), dma((2,))],
    )(*outs)


def solution(mesh):
    placed = (
        P("ep", "tp"), P("ep", "tp"), P("ep", "tp"), P("ep", "tp"),
        P("tp"), P("tp"), P("tp", None), P("ep", None), P(),
        P("ep", None), P("ep", None),
        P("ep", None, "tp"), P("ep", None, "tp"), P("ep", None, "tp"),
    )
    return jax.shard_map(
        body,
        mesh=mesh,
        in_specs=placed,
        out_specs=(P(("ep", "tp"), None), P("ep", "tp")),
        check_vma=False,
    )
```

```python
import functools

import jax
import jax.numpy as jnp
import numpy as np
from jax import lax
from jax.experimental import pallas as pl
from jax.experimental.pallas import tpu as pltpu
from jax.sharding import PartitionSpec as P

epsilon = 1e-06
rope_base = 10000.0
VMEM_LIMIT = 56 * 2**20
UNITS, PIECES, SHARES = 8, 2, 2
GROUPS = tuple((u,) for u in range(UNITS))
F32 = jnp.float32
BF16 = jnp.bfloat16
MESH = pl.DeviceIdType.MESH


def dot(a, b):
    return jnp.dot(a, b, preferred_element_type=F32)


def iota(shape, dim):
    return lax.broadcasted_iota(jnp.int32, shape, dim)


def silu(v):
    return v / (1.0 + jnp.exp(-v))


def kernel(
    size,
    ids_h, tok_h, tgain_h, wg_h, wu_h, query_h, key_h, value_h, decay_h, freq_h, sign_h,
    rweights_h, gate_h, hgain_h, ow_h, wd_h,
    ret_out, exp_out,
    ids_t, tok, tgain, wg, wu, query, key, value, decay, freq, turn_sign,
    rweights_t, gate, hgain, ow, wd,
    normed, raw, ids_in, far_picks, obuf, xbuf, hbuf, gate_acc, up_acc, sbuf, rbuf, w_hi, w_lo, cos_t, sin_t,
    rq, rk, local, state, total_state, st_send, st_recv, mixed, part, rs1, rs2_send, rs2_recv,
    load_sem, id_send, id_recv, raw_send, raw_recv, ry_send, ry_recv, d_send, d_recv, xc_send, xc_recv,
    hy_send, hy_recv, hc_send, hc_recv, b_send, b_recv, st_ssem, st_rsem,
    r1_send, r1_recv, r2_send, r2_recv,
):
    ep, tp, cap, rounds, per, groups = (
        size["ep"], size["tp"], size["cap"], size["rounds"], size["per"], size["groups"]
    )
    ys = tp // 2
    e, t = lax.axis_index("ep"), lax.axis_index("tp")
    y, c = t // 2, lax.rem(t, 2)
    mate = (e, y * 2 + 1 - c)
    heads = decay.shape[0]
    tokens, model = tok.shape
    half = model // 2
    block_len = query.shape[0]
    dk = query.shape[1] // heads

    def bit(b):
        return lax.rem(e // 2**b, 2)

    def flipped(k):
        out = e
        for b in range(rounds):
            if k >> b & 1:
                out = out + (1 - 2 * bit(b)) * 2**b
        return out

    def pair(k):
        return (flipped(k), t)

    def y_at(offset):
        return lax.rem(y + offset, ys)

    def over_y(offset):
        return (e, y_at(offset) * 2 + c)

    def remote(src, dst, ssem, rsem, device):
        return pltpu.make_async_remote_copy(
            src_ref=src, dst_ref=dst, send_sem=ssem, recv_sem=rsem,
            device_id=device, device_id_type=MESH,
        )

    sent = []

    def send(src, dst, ssem, rsem, device):
        copy = remote(src, dst, ssem, rsem, device)
        copy.start()
        sent.append(copy)

    def arrived(dst, ssem, rsem, device):
        remote(dst, dst, ssem, rsem, device).wait_recv()

    low, top = (pl.ds(i * (wg.shape[1] // 2), wg.shape[1] // 2) for i in range(2))
    loads = {
        name: pltpu.make_async_copy(a, b, load_sem.at[i])
        for i, (name, a, b) in enumerate((
            ("ids", ids_h, ids_t), ("tok", tok_h, tok), ("tgain", tgain_h, tgain),
            ("wg0", wg_h.at[:, low], wg.at[:, low]), ("wu0", wu_h.at[:, low], wu.at[:, low]),
            ("wg1", wg_h.at[:, top], wg.at[:, top]), ("wu1", wu_h.at[:, top], wu.at[:, top]),
            ("query", query_h, query), ("key", key_h, key),
            ("value", value_h, value), ("decay", decay_h, decay), ("freq", freq_h, freq),
            ("sign", sign_h, turn_sign), ("rweights", rweights_h, rweights_t),
            ("gate", gate_h, gate), ("hgain", hgain_h, hgain), ("ow", ow_h, ow), ("wd", wd_h, wd)))
    }
    for copy in loads.values():
        copy.start()

    barrier = pltpu.get_barrier_semaphore()
    friends = [pair(k) for k in range(1, ep)] + [over_y(i) for i in range(1, ys)] + [mate]
    for friend in friends:
        pl.semaphore_signal(barrier, inc=1, device_id=friend, device_id_type=MESH)

    rows = max(ep, 16)
    after = jnp.where(
        iota((tokens, tokens), 0) < iota((tokens, tokens), 1), 1.0, 0.0).astype(BF16)

    def positions(ids):
        rel = jnp.bitwise_xor(ids, e)
        named = [iota((rows, tokens), 0) == rel[i:i + 1, :] for i in range(2)]
        rank = dot(jnp.where(named[0] | named[1], 1.0, 0.0).astype(BF16), after)
        return [
            rel[i:i + 1, :] * cap + jnp.sum(
                jnp.where(named[i], rank, 0.0), 0, keepdims=True).astype(jnp.int32)
            for i in range(2)
        ]

    def picks(pos, k, n):
        row_id = k * cap + iota((n * cap, tokens), 0)
        return jnp.where((row_id == pos[0]) | (row_id == pos[1]), 1.0, 0.0).astype(BF16)

    loads["ids"].wait()
    pos_t = positions(ids_t[...])
    loads["tok"].wait()
    loads["tgain"].wait()
    rows_float = tok[...].astype(F32)
    scale = lax.rsqrt(jnp.mean(rows_float * rows_float, -1, keepdims=True) + epsilon)
    normed[...] = (rows_float * scale * tgain[...]).astype(BF16)

    def block(j, n=1):
        return pl.ds(j * cap, n * cap)

    def unit(u, n=1):
        return block(u * per, n * per)

    mine = pl.ds(pl.multiple_of(c * half, half), half)
    def blocks(u):
        return [k for k in range(u * per, (u + 1) * per) if k > 0]

    units = ep // per
    far, near = ep // 2, units // 2
    pieces = size["pieces"]
    shares = min(SHARES, pieces)
    width = half // pieces
    strip = width // ys

    def piece(i):
        return pl.ds(i * width, width)

    def strip_cols(i, at):
        return pl.ds(pl.multiple_of(i * width + at * strip, strip), strip)

    def push(u):
        obuf[unit(u), :] = dot(picks(pos_t, u * per, per), normed[:, mine]).astype(BF16)
        for k in blocks(u):
            send(obuf.at[block(k)], xbuf.at[c, block(k)], d_send.at[k, 0], d_recv.at[k, 0],
                 pair(k))

    def raw_push(i):
        if i == 0:
            send(ids_t, ids_in, id_send.at[0], id_recv.at[0], pair(far))
        shared = i < shares
        begin = c * half + i * width + (y * strip if shared else 0)
        size_of = strip if shared else width
        cols = pl.ds(pl.multiple_of(begin, size_of), size_of)
        there = strip_cols(i, y) if shared else piece(i)
        send(normed.at[:, cols], raw.at[:, there], raw_send.at[i], raw_recv.at[i], pair(far))

    def raw_relay(i):
        if i >= shares:
            return
        ref = raw.at[:, strip_cols(i, y)]
        arrived(ref, raw_send.at[i], raw_recv.at[i], pair(far))
        for a in range(1, ys):
            send(ref, ref, ry_send.at[a, i], ry_recv.at[a, i], over_y(a))

    def far_select(i):
        if i == 0:
            arrived(ids_in, id_send.at[0], id_recv.at[0], pair(far))
            far_picks[...] = picks(positions(ids_in[...]), 0, far)
        if i >= shares:
            arrived(raw.at[:, piece(i)], raw_send.at[i], raw_recv.at[i], pair(far))
        for a in range(1, ys if i < shares else 1):
            arrived(raw.at[:, strip_cols(i, y_at(ys - a))], ry_send.at[a, i], ry_recv.at[a, i],
                    over_y(a))
        for u in range(near):
            chosen = dot(far_picks[unit(u), :], raw[:, piece(i)]).astype(BF16)
            obuf[unit(near + u), piece(i)] = chosen
            if u == 0:
                xbuf[c, block(far), piece(i)] = chosen[:cap]
            for k in blocks(u):
                j = far + k
                send(obuf.at[block(j), piece(i)], xbuf.at[c, block(j), piece(i)],
                     d_send.at[j, i], d_recv.at[j, i], pair(k))

    def landed(u):
        for k in blocks(u):
            if k < far:
                arrived(xbuf.at[c, block(k)], d_send.at[k, 0], d_recv.at[k, 0], pair(k))
            elif k > far:
                for i in range(pieces):
                    arrived(xbuf.at[c, block(k), piece(i)], d_send.at[k, i], d_recv.at[k, i],
                            pair(k - far))

    def x_relay(u):
        if not blocks(u):
            return
        landed(u)
        send(xbuf.at[c, unit(u)], xbuf.at[c, unit(u)], xc_send.at[u], xc_recv.at[u], mate)

    def own_block():
        if per == 1:
            own = picks(pos_t, 0, 1)
            for i in range(2):
                xbuf[i, block(0), :] = dot(own, normed[:, pl.ds(i * half, half)]).astype(BF16)
        else:
            xbuf[c, block(0), :] = obuf[block(0), :]

    pl.semaphore_wait(barrier, len(friends))
    def x_collect(u):
        if not blocks(u):
            return
        arrived(xbuf.at[1 - c, unit(u)], xc_send.at[u], xc_recv.at[u], mate)

    ff = wg.shape[1]
    n_tile = min(256, ff // 2)

    def group_rows(g):
        return unit(groups[g][0], len(groups[g]))

    def up(g, first=0, stop=None):
        for u in groups[g]:
            x_collect(u)
        rws = group_rows(g)

        def tile(n, carry):
            cols = pl.ds(pl.multiple_of(n * n_tile, n_tile), n_tile)
            a = v = None
            for p in range(2):
                x = xbuf[p, rws, :]
                ins = pl.ds(p * half, half)
                gp, vp = dot(x, wg[ins, cols]), dot(x, wu[ins, cols])
                a, v = (gp, vp) if a is None else (a + gp, v + vp)
            hbuf[t, rws, cols] = (silu(a) * v).astype(BF16)
            return carry

        lax.fori_loop(first, ff // n_tile if stop is None else stop, tile, 0)

    def up_half(g, core):
        ins = pl.ds(pl.multiple_of(core * half, half), half)
        rws = group_rows(g)

        def products(n):
            cols = pl.ds(pl.multiple_of(n * n_tile, n_tile), n_tile)
            x = xbuf[core, rws, :]
            return cols, dot(x, wg[ins, cols]), dot(x, wu[ins, cols])

        return rws, products

    def up_mine(g):
        rws, products = up_half(g, c)

        def tile(n, carry):
            cols, a, v = products(n)
            gate_acc[:, cols] = a
            up_acc[:, cols] = v
            return carry

        lax.fori_loop(0, ff // n_tile, tile, 0)

    def up_rest(g):
        for u in groups[g]:
            x_collect(u)
        rws, products = up_half(g, 1 - c)

        def tile(n, carry):
            cols, a, v = products(n)
            hbuf[t, rws, cols] = (silu(gate_acc[:, cols] + a) * (up_acc[:, cols] + v)).astype(BF16)
            return carry

        lax.fori_loop(0, ff // n_tile, tile, 0)

    def up_send(g):
        rws = group_rows(g)
        for a in range(1, ys):
            send(hbuf.at[t, rws], hbuf.at[t, rws], hy_send.at[a, g], hy_recv.at[a, g], over_y(a))
        send(hbuf.at[t, rws], hbuf.at[t, rws], hc_send.at[0, g], hc_recv.at[0, g], mate)

    def h_pass(g):
        rws = group_rows(g)
        for a in range(1, ys):
            piece = y_at(ys - a) * 2 + c
            arrived(hbuf.at[piece, rws], hy_send.at[a, g], hy_recv.at[a, g], over_y(a))
            send(hbuf.at[piece, rws], hbuf.at[piece, rws], hc_send.at[a, g], hc_recv.at[a, g],
                 mate)

    cw = wd.shape[1]
    d_tile = min(256, cw)

    def down(g):
        rws = group_rows(g)
        for a in range(ys):
            piece = y_at(ys - a) * 2 + 1 - c
            arrived(hbuf.at[piece, rws], hc_send.at[a, g], hc_recv.at[a, g], mate)

        def tile(n, carry):
            cols = pl.ds(pl.multiple_of(n * d_tile, d_tile), d_tile)
            total = None
            for p in range(tp):
                now = dot(hbuf[p, rws, :], wd[pl.ds(p * ff, ff), cols])
                total = now if total is None else total + now
            sbuf[rws, cols] = total.astype(BF16)
            return carry

        lax.fori_loop(0, cw // d_tile, tile, 0)
        for u in groups[g]:
            for k in range(u * per, (u + 1) * per):
                if k > 0:
                    send(sbuf.at[block(k)], rbuf.at[block(k)], b_send.at[k], b_recv.at[k], pair(k))
                else:
                    rbuf[block(0), :] = sbuf[block(0), :]

    within = iota((block_len, 1), 0).astype(F32)

    def head_cols(h):
        return pl.ds(pl.multiple_of(h * dk, dk), dk)

    def turn(x):
        return x * cos_t[...] + pltpu.roll(x, dk // 2, 1) * sin_t[...]

    def states():
        for name in ("query", "key", "value", "decay", "freq", "sign"):
            loads[name].wait()
        angles = (e * block_len + iota((block_len, dk), 0)).astype(F32) * freq[...]
        cos_t[...] = jnp.cos(angles)
        sin_t[...] = jnp.sin(angles) * turn_sign[...]

        def one(h, carry):
            cols = head_cols(h)
            rate = decay[h]
            rq[:, cols] = turn(query[:, cols].astype(F32)).astype(BF16)
            rot_key = (turn(key[:, cols].astype(F32)) * dk ** (-0.5)).astype(BF16)
            rk[:, cols] = rot_key
            decayed = (rot_key.astype(F32) * jnp.exp(-rate * (block_len - 1.0 - within))).astype(BF16)
            now = lax.dot_general(
                decayed, value[:, cols], (((0,), (0,)), ((), ())), preferred_element_type=F32)
            total_state[h] = now
            state[h] = jnp.zeros((dk, dk), F32)
            return carry

        lax.fori_loop(0, heads, one, 0)

    def lane(h, times):
        return jnp.exp(jnp.full((1, dk), -decay[h] * (block_len * times), F32))

    last = rounds - 1

    def state_copy(r):
        return remote(st_send.at[r], st_recv.at[r], st_ssem.at[r], st_rsem.at[r], pair(2**r))

    def state_send(r):
        def one(h, carry):
            st_send[r, h] = total_state[h].astype(BF16)
            return carry

        lax.fori_loop(0, heads, one, 0)
        if r < last:
            copy = state_copy(r)
            copy.start()
            sent.append(copy)
        else:
            @pl.when(bit(r) == 0)
            def _():
                state_copy(r).start()

    def state_take(r):
        later = bit(r) == 1
        before = lax.rem(e, 2**r).astype(F32)

        def one(h, carry):
            got = st_recv[r, h].astype(F32)
            state[h] = state[h] + jnp.where(later, got * lane(h, before), 0.0)
            if r < last:
                far = lane(h, float(2**r))
                total_state[h] = jnp.where(
                    later, got * far + total_state[h], total_state[h] * far + got)
            return carry

        def take():
            state_copy(r).wait_recv()
            lax.fori_loop(0, heads, one, 0)

        if r < last:
            take()
        else:
            pl.when(later)(take)

    def combine_weights():
        diagonal = iota((tokens, tokens), 0) == iota((tokens, tokens), 1)

        def upright(row):
            return jnp.sum(jnp.where(diagonal, row, 0.0), 1, keepdims=True)

        col = iota((tokens, ep * cap), 1)
        pos0 = upright(pos_t[0].astype(F32)).astype(jnp.int32)
        pos1 = upright(pos_t[1].astype(F32)).astype(jnp.int32)
        weight = jnp.where(col == pos0, upright(rweights_t[0:1, :]), 0.0) + jnp.where(
            col == pos1, upright(rweights_t[1:2, :]), 0.0)
        high = weight.astype(BF16)
        w_hi[...] = high
        w_lo[...] = (weight - high.astype(F32)).astype(BF16)

    chunk = min(128, block_len)

    chunks = block_len // chunk

    def head_local(first, stop):
        def one(h, carry):
            cols = head_cols(h)
            rate = decay[h]
            key_grow = jnp.exp(rate * iota((1, block_len), 1).astype(F32))
            for i in range(chunks):
                seen_keys = (i + 1) * chunk
                rws, keys = pl.ds(i * chunk, chunk), pl.ds(0, seen_keys)
                place = i * chunk + iota((chunk, 1), 0)
                scores = lax.dot_general(
                    rq[rws, cols], rk[keys, cols], (((1,), (1,)), ((), ())),
                    preferred_element_type=F32)
                fade = jnp.exp(-rate * place.astype(F32)) * key_grow[:, :seen_keys]
                seen = iota((chunk, seen_keys), 1) <= place
                weights = jnp.where(seen, scores * fade, 0.0).astype(BF16)
                local[rws, cols] = dot(weights, value[keys, cols])
            return carry

        lax.fori_loop(first, stop, one, 0)

    def finish(first, stop):
        def one(h, carry):
            cols = head_cols(h)
            held = state[h]
            high = held.astype(BF16)
            low = (held - high.astype(F32)).astype(BF16)
            for i in range(chunks):
                rws = pl.ds(i * chunk, chunk)
                place = (i * chunk + iota((chunk, 1), 0)).astype(F32)
                q = rq[rws, cols]
                retained = local[rws, cols] + (dot(q, high) + dot(q, low)) * jnp.exp(
                    -decay[h] * (place + 1.0))
                centered = retained - jnp.mean(retained, -1, keepdims=True)
                out = centered * lax.rsqrt(
                    jnp.mean(centered * centered, -1, keepdims=True) + epsilon)
                mixed[rws, cols] = (
                    out * hgain[:, cols] * silu(gate[rws, cols].astype(F32))).astype(BF16)
            return carry

        lax.fori_loop(first, stop, one, 0)

    rb = block_len // tp
    o_tile = min(512, model)

    def project():
        def step(n, carry):
            cols = pl.ds(pl.multiple_of(n * o_tile, o_tile), o_tile)
            for d in range(tp):
                part[d, :, cols] = dot(mixed[pl.ds(d * rb, rb), :], ow[:, cols]).astype(BF16)
            return carry

        lax.fori_loop(0, model // o_tile, step, 0)
        for b in range(ys):
            send(part.at[b * 2 + 1 - c], rs1.at[b], r1_send.at[b], r1_recv.at[b], mate)

    def sum_over_cores():
        for b in range(ys):
            arrived(rs1.at[b], r1_send.at[b], r1_recv.at[b], mate)
        for a in range(1, ys):
            b = y_at(a)
            rs2_send[a - 1] = (part[b * 2 + c].astype(F32) + rs1[b].astype(F32)).astype(BF16)
            send(rs2_send.at[a - 1], rs2_recv.at[a - 1], r2_send.at[a - 1], r2_recv.at[a - 1],
                 over_y(a))

    if blocks(0):
        push(0)
    for u in range(1, near):
        push(u)
    own_block()
    loads["wg0"].wait()
    loads["wu0"].wait()
    x_relay(0)
    parts = ff // n_tile
    if blocks(0):
        loads["wg1"].wait()
        loads["wu1"].wait()
        up(0)
    else:
        up(0, 0, parts // 2)
        loads["wg1"].wait()
        loads["wu1"].wait()
        up(0, parts // 2, parts)
    up_send(0)
    states()
    state_send(0)
    x_relay(1)
    for i in range(pieces):
        raw_push(i)
    up_mine(1)
    x_relay(2)
    up_rest(1)
    up_send(1)
    h_pass(0)
    head_local(0, heads)
    raw_relay(0)
    up(2)
    for i in range(1, pieces):
        raw_relay(i)
    up_send(2)
    state_take(0)
    state_send(1)
    x_relay(3)
    h_pass(1)
    far_select(0)
    up(3)
    up_send(3)
    loads["wd"].wait()
    down(0)
    for i in range(1, pieces):
        far_select(i)
    x_relay(4)
    up_mine(4)
    state_take(1)
    state_send(2)
    h_pass(2)
    up_rest(4)
    up_send(4)
    x_relay(5)
    x_relay(6)
    down(1)
    up(5)
    up_send(5)
    h_pass(3)
    for r in range(3, rounds):
        state_take(r - 1)
        state_send(r)
    x_relay(7)
    state_take(last)
    loads["gate"].wait()
    loads["hgain"].wait()
    loads["ow"].wait()
    finish(0, heads)
    up(6)
    up_send(6)
    h_pass(4)
    project()
    up(7)
    up_send(7)
    early = len(sent)
    down(4)
    h_pass(5)
    sum_over_cores()
    down(5)
    h_pass(6)
    down(2)
    down(6)
    down(3)
    loads["rweights"].wait()
    combine_weights()
    h_pass(7)
    down(7)

    for copy in sent[:early]:
        copy.wait_send()
    split = ep // 2
    for k in range(1, split):
        arrived(rbuf.at[block(k)], b_send.at[k], b_recv.at[k], pair(k))

    def weighed(cols):
        rows_back = rbuf[cols, :]
        return dot(w_hi[:, cols], rows_back) + dot(w_lo[:, cols], rows_back)

    close = weighed(block(0, split))
    total = part[t].astype(F32) + rs1[y].astype(F32)
    for a in range(1, ys):
        arrived(rs2_recv.at[a - 1], r2_send.at[a - 1], r2_recv.at[a - 1], over_y(a))
        total += rs2_recv[a - 1].astype(F32)
    ret_out[...] = total.astype(BF16)
    for k in range(split, ep):
        arrived(rbuf.at[block(k)], b_send.at[k], b_recv.at[k], pair(k))
    exp_out[...] = (close + weighed(block(split, ep - split))).astype(BF16)
    for copy in sent[early:]:
        copy.wait_send()

    @pl.when(bit(last) == 0)
    def _():
        state_copy(last).wait_send()


def body(
    query_in, key_in, value_in, gate_in, decay_rate, head_gain, output_weight,
    token_rows, token_gain, route_ids, route_weights, expert_gate, expert_up, expert_down,
):
    ep, tp = lax.axis_size("ep"), lax.axis_size("tp")
    tokens, model = token_rows.shape
    top = route_ids.shape[1]
    cap = -(-(2 * tokens * top // ep) // 32) * 32
    block_len, width = query_in.shape
    heads = decay_rate.shape[0]
    dk = width // heads
    ff = expert_gate.shape[2]
    cw = expert_down.shape[2]
    ys = tp // 2
    rounds = ep.bit_length() - 1
    assert ep == 2**rounds and rounds >= 3
    per = ep // UNITS
    pieces = max(1, min(PIECES, model // (2 * 128 * ys)))
    turns = dk // 2
    freq = np.tile(
        np.float32(rope_base) ** (-np.arange(turns, dtype=np.float32) * np.float32(2.0 / dk)), 2)
    turn_sign = np.where(np.arange(dk) < turns, -1.0, 1.0)
    size = dict(ep=ep, tp=tp, cap=cap, rounds=rounds, per=per, groups=GROUPS, pieces=pieces)
    slots = ep * cap
    rb = block_len // tp
    hbm = pl.BlockSpec(memory_space=pl.ANY)
    vmem = pl.BlockSpec(memory_space=pltpu.VMEM)
    dma = pltpu.SemaphoreType.DMA
    given = [
        route_ids.T, token_rows, token_gain[None, :], expert_gate[0], expert_up[0],
        query_in, key_in, value_in, decay_rate,
        jnp.asarray(freq[None, :], F32), jnp.asarray(turn_sign[None, :], F32),
        route_weights.T, gate_in, head_gain[None, :], output_weight, expert_down[0],
    ]
    nm = len(GROUPS)
    outs = pl.pallas_call(
        functools.partial(kernel, size),
        out_shape=(pltpu.VMEM((rb, model), BF16), pltpu.VMEM((tokens, cw), BF16)),
        in_specs=[hbm] * len(given),
        out_specs=(vmem, vmem),
        scratch_shapes=[
            (pltpu.SMEM if a is decay_rate else pltpu.VMEM)(a.shape, a.dtype) for a in given]
        + [
            pltpu.VMEM((tokens, model), BF16),
            pltpu.VMEM((tokens, model // 2), BF16),
            pltpu.VMEM((top, tokens), jnp.int32),
            pltpu.VMEM((slots // 2, tokens), BF16),
            pltpu.VMEM((slots, model // 2), BF16),
            pltpu.VMEM((2, slots, model // 2), BF16),
            pltpu.VMEM((tp, slots, ff), BF16),
            pltpu.VMEM((per * cap, ff), F32),
            pltpu.VMEM((per * cap, ff), F32),
            pltpu.VMEM((slots, cw), BF16),
            pltpu.VMEM((slots, cw), BF16),
            pltpu.VMEM((tokens, slots), BF16),
            pltpu.VMEM((tokens, slots), BF16),
            pltpu.VMEM((block_len, dk), F32),
            pltpu.VMEM((block_len, dk), F32),
            pltpu.VMEM((block_len, width), BF16),
            pltpu.VMEM((block_len, width), BF16),
            pltpu.VMEM((block_len, width), F32),
            pltpu.VMEM((heads, dk, dk), F32),
            pltpu.VMEM((heads, dk, dk), F32),
            pltpu.VMEM((rounds, heads, dk, dk), BF16),
            pltpu.VMEM((rounds, heads, dk, dk), BF16),
            pltpu.VMEM((block_len, width), BF16),
            pltpu.VMEM((tp, rb, model), BF16),
            pltpu.VMEM((ys, rb, model), BF16),
            pltpu.VMEM((max(ys - 1, 1), rb, model), BF16),
            pltpu.VMEM((max(ys - 1, 1), rb, model), BF16),
            dma((len(given) + 2,)),
            dma((1,)), dma((1,)), dma((pieces,)), dma((pieces,)),
            dma((ys, pieces)), dma((ys, pieces)),
            dma((ep, pieces)), dma((ep, pieces)),
            dma((UNITS,)), dma((UNITS,)),
            dma((ys, nm)), dma((ys, nm)), dma((ys, nm)), dma((ys, nm)),
            dma((ep,)), dma((ep,)),
            dma((rounds,)), dma((rounds,)),
            dma((ys,)), dma((ys,)), dma((ys,)), dma((ys,)),
        ],
        compiler_params=pltpu.CompilerParams(
            collective_id=0, has_side_effects=True, vmem_limit_bytes=VMEM_LIMIT
        ),
    )(*given)
    return outs


def solution(mesh):
    placed = (
        P("ep", "tp"), P("ep", "tp"), P("ep", "tp"), P("ep", "tp"),
        P("tp"), P("tp"), P("tp", None), P("ep", None), P(),
        P("ep", None), P("ep", None),
        P("ep", None, "tp"), P("ep", None, "tp"), P("ep", None, "tp"),
    )
    return jax.shard_map(
        body,
        mesh=mesh,
        in_specs=placed,
        out_specs=(P(("ep", "tp"), None), P("ep", "tp")),
        check_vma=False,
    )
```

```python
import functools

import jax
import jax.numpy as jnp
import numpy as np
from jax import lax
from jax.experimental import pallas as pl
from jax.experimental.pallas import tpu as pltpu
from jax.sharding import PartitionSpec as P

epsilon = 1e-06
rope_base = 10000.0
VMEM_LIMIT = 56 * 2**20
UNITS, PIECES, SHARES = 8, 2, 2
GROUPS = tuple((u,) for u in range(UNITS))
F32 = jnp.float32
BF16 = jnp.bfloat16
MESH = pl.DeviceIdType.MESH


def dot(a, b):
    return jnp.dot(a, b, preferred_element_type=F32)


def iota(shape, dim):
    return lax.broadcasted_iota(jnp.int32, shape, dim)


def silu(v):
    return v / (1.0 + jnp.exp(-v))


def kernel(
    size,
    ids_h, tok_h, tgain_h, wg_h, wu_h, query_h, key_h, value_h, decay_h, freq_h, sign_h,
    rweights_h, gate_h, hgain_h, ow_h, wd_h,
    ret_out, exp_out,
    ids_t, tok, tgain, wg, wu, query, key, value, decay, freq, turn_sign,
    rweights_t, gate, hgain, ow, wd,
    normed, raw, ids_in, far_picks, obuf, xbuf, hbuf, gate_acc, up_acc, sbuf, rbuf, w_hi, w_lo, cos_t, sin_t,
    rq, rk, local, state, total_state, st_send, st_recv, mixed, part, rs1, rs2_send, rs2_recv,
    load_sem, id_send, id_recv, raw_send, raw_recv, ry_send, ry_recv, d_send, d_recv, xc_send, xc_recv,
    hy_send, hy_recv, hc_send, hc_recv, b_send, b_recv, st_ssem, st_rsem,
    r1_send, r1_recv, r2_send, r2_recv,
):
    ep, tp, cap, rounds, per, groups = (
        size["ep"], size["tp"], size["cap"], size["rounds"], size["per"], size["groups"]
    )
    ys = tp // 2
    e, t = lax.axis_index("ep"), lax.axis_index("tp")
    y, c = t // 2, lax.rem(t, 2)
    mate = (e, y * 2 + 1 - c)
    heads = decay.shape[0]
    tokens, model = tok.shape
    half = model // 2
    block_len = query.shape[0]
    dk = query.shape[1] // heads

    def bit(b):
        return lax.rem(e // 2**b, 2)

    def flipped(k):
        out = e
        for b in range(rounds):
            if k >> b & 1:
                out = out + (1 - 2 * bit(b)) * 2**b
        return out

    def pair(k):
        return (flipped(k), t)

    def y_at(offset):
        return lax.rem(y + offset, ys)

    def over_y(offset):
        return (e, y_at(offset) * 2 + c)

    def remote(src, dst, ssem, rsem, device):
        return pltpu.make_async_remote_copy(
            src_ref=src, dst_ref=dst, send_sem=ssem, recv_sem=rsem,
            device_id=device, device_id_type=MESH,
        )

    sent = []

    def send(src, dst, ssem, rsem, device):
        copy = remote(src, dst, ssem, rsem, device)
        copy.start()
        sent.append(copy)

    def arrived(dst, ssem, rsem, device):
        remote(dst, dst, ssem, rsem, device).wait_recv()

    low, top = (pl.ds(i * (wg.shape[1] // 2), wg.shape[1] // 2) for i in range(2))
    loads = {
        name: pltpu.make_async_copy(a, b, load_sem.at[i])
        for i, (name, a, b) in enumerate((
            ("ids", ids_h, ids_t), ("tok", tok_h, tok), ("tgain", tgain_h, tgain),
            ("wg0", wg_h.at[:, low], wg.at[:, low]), ("wu0", wu_h.at[:, low], wu.at[:, low]),
            ("wg1", wg_h.at[:, top], wg.at[:, top]), ("wu1", wu_h.at[:, top], wu.at[:, top]),
            ("query", query_h, query), ("key", key_h, key),
            ("value", value_h, value), ("decay", decay_h, decay), ("freq", freq_h, freq),
            ("sign", sign_h, turn_sign), ("rweights", rweights_h, rweights_t),
            ("gate", gate_h, gate), ("hgain", hgain_h, hgain), ("ow", ow_h, ow), ("wd", wd_h, wd)))
    }
    for copy in loads.values():
        copy.start()

    barrier = pltpu.get_barrier_semaphore()
    friends = [pair(k) for k in range(1, ep)] + [over_y(i) for i in range(1, ys)] + [mate]
    for friend in friends:
        pl.semaphore_signal(barrier, inc=1, device_id=friend, device_id_type=MESH)

    rows = max(ep, 16)
    after = jnp.where(
        iota((tokens, tokens), 0) < iota((tokens, tokens), 1), 1.0, 0.0).astype(BF16)

    def positions(ids):
        rel = jnp.bitwise_xor(ids, e)
        named = [iota((rows, tokens), 0) == rel[i:i + 1, :] for i in range(2)]
        rank = dot(jnp.where(named[0] | named[1], 1.0, 0.0).astype(BF16), after)
        return [
            rel[i:i + 1, :] * cap + jnp.sum(
                jnp.where(named[i], rank, 0.0), 0, keepdims=True).astype(jnp.int32)
            for i in range(2)
        ]

    def picks(pos, k, n):
        row_id = k * cap + iota((n * cap, tokens), 0)
        return jnp.where((row_id == pos[0]) | (row_id == pos[1]), 1.0, 0.0).astype(BF16)

    loads["ids"].wait()
    pos_t = positions(ids_t[...])
    loads["tok"].wait()
    loads["tgain"].wait()
    rows_float = tok[...].astype(F32)
    scale = lax.rsqrt(jnp.mean(rows_float * rows_float, -1, keepdims=True) + epsilon)
    normed[...] = (rows_float * scale * tgain[...]).astype(BF16)

    def block(j, n=1):
        return pl.ds(j * cap, n * cap)

    def unit(u, n=1):
        return block(u * per, n * per)

    mine = pl.ds(pl.multiple_of(c * half, half), half)
    def blocks(u):
        return [k for k in range(u * per, (u + 1) * per) if k > 0]

    units = ep // per
    far, near = ep // 2, units // 2
    pieces = size["pieces"]
    shares = min(SHARES, pieces)
    width = half // pieces
    strip = width // ys

    def piece(i):
        return pl.ds(i * width, width)

    def strip_cols(i, at):
        return pl.ds(pl.multiple_of(i * width + at * strip, strip), strip)

    def push(u):
        obuf[unit(u), :] = dot(picks(pos_t, u * per, per), normed[:, mine]).astype(BF16)
        for k in blocks(u):
            send(obuf.at[block(k)], xbuf.at[c, block(k)], d_send.at[k, 0], d_recv.at[k, 0],
                 pair(k))

    def raw_push(i):
        if i == 0:
            send(ids_t, ids_in, id_send.at[0], id_recv.at[0], pair(far))
        shared = i < shares
        begin = c * half + i * width + (y * strip if shared else 0)
        size_of = strip if shared else width
        cols = pl.ds(pl.multiple_of(begin, size_of), size_of)
        there = strip_cols(i, y) if shared else piece(i)
        send(normed.at[:, cols], raw.at[:, there], raw_send.at[i], raw_recv.at[i], pair(far))

    def raw_relay(i):
        if i >= shares:
            return
        ref = raw.at[:, strip_cols(i, y)]
        arrived(ref, raw_send.at[i], raw_recv.at[i], pair(far))
        for a in range(1, ys):
            send(ref, ref, ry_send.at[a, i], ry_recv.at[a, i], over_y(a))

    def far_select(i):
        if i == 0:
            arrived(ids_in, id_send.at[0], id_recv.at[0], pair(far))
            far_picks[...] = picks(positions(ids_in[...]), 0, far)
        if i >= shares:
            arrived(raw.at[:, piece(i)], raw_send.at[i], raw_recv.at[i], pair(far))
        for a in range(1, ys if i < shares else 1):
            arrived(raw.at[:, strip_cols(i, y_at(ys - a))], ry_send.at[a, i], ry_recv.at[a, i],
                    over_y(a))
        for u in range(near):
            chosen = dot(far_picks[unit(u), :], raw[:, piece(i)]).astype(BF16)
            obuf[unit(near + u), piece(i)] = chosen
            if u == 0:
                xbuf[c, block(far), piece(i)] = chosen[:cap]
            for k in blocks(u):
                j = far + k
                send(obuf.at[block(j), piece(i)], xbuf.at[c, block(j), piece(i)],
                     d_send.at[j, i], d_recv.at[j, i], pair(k))

    def landed(u):
        for k in blocks(u):
            if k < far:
                arrived(xbuf.at[c, block(k)], d_send.at[k, 0], d_recv.at[k, 0], pair(k))
            elif k > far:
                for i in range(pieces):
                    arrived(xbuf.at[c, block(k), piece(i)], d_send.at[k, i], d_recv.at[k, i],
                            pair(k - far))

    def x_relay(u):
        if not blocks(u):
            return
        landed(u)
        send(xbuf.at[c, unit(u)], xbuf.at[c, unit(u)], xc_send.at[u], xc_recv.at[u], mate)

    def own_block():
        if per == 1:
            own = picks(pos_t, 0, 1)
            for i in range(2):
                xbuf[i, block(0), :] = dot(own, normed[:, pl.ds(i * half, half)]).astype(BF16)
        else:
            xbuf[c, block(0), :] = obuf[block(0), :]

    pl.semaphore_wait(barrier, len(friends))
    def x_collect(u):
        if not blocks(u):
            return
        arrived(xbuf.at[1 - c, unit(u)], xc_send.at[u], xc_recv.at[u], mate)

    ff = wg.shape[1]
    n_tile = min(256, ff // 2)

    def group_rows(g):
        return unit(groups[g][0], len(groups[g]))

    def up(g, first=0, stop=None):
        for u in groups[g]:
            x_collect(u)
        rws = group_rows(g)

        def tile(n, carry):
            cols = pl.ds(pl.multiple_of(n * n_tile, n_tile), n_tile)
            a = v = None
            for p in range(2):
                x = xbuf[p, rws, :]
                ins = pl.ds(p * half, half)
                gp, vp = dot(x, wg[ins, cols]), dot(x, wu[ins, cols])
                a, v = (gp, vp) if a is None else (a + gp, v + vp)
            hbuf[t, rws, cols] = (silu(a) * v).astype(BF16)
            return carry

        lax.fori_loop(first, ff // n_tile if stop is None else stop, tile, 0)

    def up_half(g, core):
        ins = pl.ds(pl.multiple_of(core * half, half), half)
        rws = group_rows(g)

        def products(n):
            cols = pl.ds(pl.multiple_of(n * n_tile, n_tile), n_tile)
            x = xbuf[core, rws, :]
            return cols, dot(x, wg[ins, cols]), dot(x, wu[ins, cols])

        return rws, products

    def up_mine(g):
        rws, products = up_half(g, c)

        def tile(n, carry):
            cols, a, v = products(n)
            gate_acc[:, cols] = a
            up_acc[:, cols] = v
            return carry

        lax.fori_loop(0, ff // n_tile, tile, 0)

    def up_rest(g):
        for u in groups[g]:
            x_collect(u)
        rws, products = up_half(g, 1 - c)

        def tile(n, carry):
            cols, a, v = products(n)
            hbuf[t, rws, cols] = (silu(gate_acc[:, cols] + a) * (up_acc[:, cols] + v)).astype(BF16)
            return carry

        lax.fori_loop(0, ff // n_tile, tile, 0)

    def up_send(g):
        rws = group_rows(g)
        for a in range(1, ys):
            send(hbuf.at[t, rws], hbuf.at[t, rws], hy_send.at[a, g], hy_recv.at[a, g], over_y(a))
        send(hbuf.at[t, rws], hbuf.at[t, rws], hc_send.at[0, g], hc_recv.at[0, g], mate)

    def h_pass(g):
        rws = group_rows(g)
        for a in range(1, ys):
            piece = y_at(ys - a) * 2 + c
            arrived(hbuf.at[piece, rws], hy_send.at[a, g], hy_recv.at[a, g], over_y(a))
            send(hbuf.at[piece, rws], hbuf.at[piece, rws], hc_send.at[a, g], hc_recv.at[a, g],
                 mate)

    cw = wd.shape[1]
    d_tile = min(256, cw)

    def down(g):
        rws = group_rows(g)
        for a in range(ys):
            piece = y_at(ys - a) * 2 + 1 - c
            arrived(hbuf.at[piece, rws], hc_send.at[a, g], hc_recv.at[a, g], mate)

        def tile(n, carry):
            cols = pl.ds(pl.multiple_of(n * d_tile, d_tile), d_tile)
            total = None
            for p in range(tp):
                now = dot(hbuf[p, rws, :], wd[pl.ds(p * ff, ff), cols])
                total = now if total is None else total + now
            sbuf[rws, cols] = total.astype(BF16)
            return carry

        lax.fori_loop(0, cw // d_tile, tile, 0)
        for u in groups[g]:
            for k in range(u * per, (u + 1) * per):
                if k > 0:
                    send(sbuf.at[block(k)], rbuf.at[block(k)], b_send.at[k], b_recv.at[k], pair(k))
                else:
                    rbuf[block(0), :] = sbuf[block(0), :]

    within = iota((block_len, 1), 0).astype(F32)

    def head_cols(h):
        return pl.ds(pl.multiple_of(h * dk, dk), dk)

    def turn(x):
        return x * cos_t[...] + pltpu.roll(x, dk // 2, 1) * sin_t[...]

    def states():
        for name in ("query", "key", "value", "decay", "freq", "sign"):
            loads[name].wait()
        angles = (e * block_len + iota((block_len, dk), 0)).astype(F32) * freq[...]
        cos_t[...] = jnp.cos(angles)
        sin_t[...] = jnp.sin(angles) * turn_sign[...]

        def one(h, carry):
            cols = head_cols(h)
            rate = decay[h]
            rq[:, cols] = turn(query[:, cols].astype(F32)).astype(BF16)
            rot_key = (turn(key[:, cols].astype(F32)) * dk ** (-0.5)).astype(BF16)
            rk[:, cols] = rot_key
            decayed = (rot_key.astype(F32) * jnp.exp(-rate * (block_len - 1.0 - within))).astype(BF16)
            now = lax.dot_general(
                decayed, value[:, cols], (((0,), (0,)), ((), ())), preferred_element_type=F32)
            total_state[h] = now
            state[h] = jnp.zeros((dk, dk), F32)
            return carry

        lax.fori_loop(0, heads, one, 0)

    def lane(h, times):
        return jnp.exp(jnp.full((1, dk), -decay[h] * (block_len * times), F32))

    last = rounds - 1

    def state_copy(r):
        return remote(st_send.at[r], st_recv.at[r], st_ssem.at[r], st_rsem.at[r], pair(2**r))

    def state_send(r):
        def one(h, carry):
            st_send[r, h] = total_state[h].astype(BF16)
            return carry

        lax.fori_loop(0, heads, one, 0)
        if r < last:
            copy = state_copy(r)
            copy.start()
            sent.append(copy)
        else:
            @pl.when(bit(r) == 0)
            def _():
                state_copy(r).start()

    def state_take(r):
        later = bit(r) == 1
        before = lax.rem(e, 2**r).astype(F32)

        def one(h, carry):
            got = st_recv[r, h].astype(F32)
            state[h] = state[h] + jnp.where(later, got * lane(h, before), 0.0)
            if r < last:
                far = lane(h, float(2**r))
                total_state[h] = jnp.where(
                    later, got * far + total_state[h], total_state[h] * far + got)
            return carry

        def take():
            state_copy(r).wait_recv()
            lax.fori_loop(0, heads, one, 0)

        if r < last:
            take()
        else:
            pl.when(later)(take)

    def combine_weights():
        diagonal = iota((tokens, tokens), 0) == iota((tokens, tokens), 1)

        def upright(row):
            return jnp.sum(jnp.where(diagonal, row, 0.0), 1, keepdims=True)

        col = iota((tokens, ep * cap), 1)
        pos0 = upright(pos_t[0].astype(F32)).astype(jnp.int32)
        pos1 = upright(pos_t[1].astype(F32)).astype(jnp.int32)
        weight = jnp.where(col == pos0, upright(rweights_t[0:1, :]), 0.0) + jnp.where(
            col == pos1, upright(rweights_t[1:2, :]), 0.0)
        high = weight.astype(BF16)
        w_hi[...] = high
        w_lo[...] = (weight - high.astype(F32)).astype(BF16)

    chunk = min(128, block_len)

    chunks = block_len // chunk

    def head_local(first, stop):
        def one(h, carry):
            cols = head_cols(h)
            rate = decay[h]
            key_grow = jnp.exp(rate * iota((1, block_len), 1).astype(F32))
            for i in range(chunks):
                seen_keys = (i + 1) * chunk
                rws, keys = pl.ds(i * chunk, chunk), pl.ds(0, seen_keys)
                place = i * chunk + iota((chunk, 1), 0)
                scores = lax.dot_general(
                    rq[rws, cols], rk[keys, cols], (((1,), (1,)), ((), ())),
                    preferred_element_type=F32)
                fade = jnp.exp(-rate * place.astype(F32)) * key_grow[:, :seen_keys]
                seen = iota((chunk, seen_keys), 1) <= place
                weights = jnp.where(seen, scores * fade, 0.0).astype(BF16)
                local[rws, cols] = dot(weights, value[keys, cols])
            return carry

        lax.fori_loop(first, stop, one, 0)

    def finish(first, stop):
        def one(h, carry):
            cols = head_cols(h)
            held = state[h]
            high = held.astype(BF16)
            low = (held - high.astype(F32)).astype(BF16)
            for i in range(chunks):
                rws = pl.ds(i * chunk, chunk)
                place = (i * chunk + iota((chunk, 1), 0)).astype(F32)
                q = rq[rws, cols]
                retained = local[rws, cols] + (dot(q, high) + dot(q, low)) * jnp.exp(
                    -decay[h] * (place + 1.0))
                centered = retained - jnp.mean(retained, -1, keepdims=True)
                out = centered * lax.rsqrt(
                    jnp.mean(centered * centered, -1, keepdims=True) + epsilon)
                mixed[rws, cols] = (
                    out * hgain[:, cols] * silu(gate[rws, cols].astype(F32))).astype(BF16)
            return carry

        lax.fori_loop(first, stop, one, 0)

    rb = block_len // tp
    o_tile = min(512, model)

    def project():
        def step(n, carry):
            cols = pl.ds(pl.multiple_of(n * o_tile, o_tile), o_tile)
            for d in range(tp):
                part[d, :, cols] = dot(mixed[pl.ds(d * rb, rb), :], ow[:, cols]).astype(BF16)
            return carry

        lax.fori_loop(0, model // o_tile, step, 0)
        for b in range(ys):
            send(part.at[b * 2 + 1 - c], rs1.at[b], r1_send.at[b], r1_recv.at[b], mate)

    def sum_over_cores():
        for b in range(ys):
            arrived(rs1.at[b], r1_send.at[b], r1_recv.at[b], mate)
        for a in range(1, ys):
            b = y_at(a)
            rs2_send[a - 1] = (part[b * 2 + c].astype(F32) + rs1[b].astype(F32)).astype(BF16)
            send(rs2_send.at[a - 1], rs2_recv.at[a - 1], r2_send.at[a - 1], r2_recv.at[a - 1],
                 over_y(a))

    if blocks(0):
        push(0)
    for u in range(1, near):
        push(u)
    own_block()
    loads["wg0"].wait()
    loads["wu0"].wait()
    x_relay(0)
    parts = ff // n_tile
    if blocks(0):
        loads["wg1"].wait()
        loads["wu1"].wait()
        up(0)
    else:
        up(0, 0, parts // 2)
        loads["wg1"].wait()
        loads["wu1"].wait()
        up(0, parts // 2, parts)
    up_send(0)
    states()
    state_send(0)
    x_relay(1)
    for i in range(pieces):
        raw_push(i)
    up_mine(1)
    up_rest(1)
    up_send(1)
    x_relay(2)
    h_pass(0)
    head_local(0, heads)
    raw_relay(0)
    up(2)
    for i in range(1, pieces):
        raw_relay(i)
    up_send(2)
    state_take(0)
    state_send(1)
    x_relay(3)
    h_pass(1)
    far_select(0)
    up(3)
    up_send(3)
    loads["wd"].wait()
    down(0)
    for i in range(1, pieces):
        far_select(i)
    x_relay(4)
    up_mine(4)
    state_take(1)
    state_send(2)
    h_pass(2)
    up_rest(4)
    up_send(4)
    x_relay(5)
    x_relay(6)
    up_mine(5)
    up_rest(5)
    up_send(5)
    h_pass(3)
    for r in range(3, rounds):
        state_take(r - 1)
        state_send(r)
    x_relay(7)
    state_take(last)
    loads["gate"].wait()
    loads["hgain"].wait()
    loads["ow"].wait()
    finish(0, heads)
    h_pass(4)
    up(6)
    up_send(6)
    project()
    down(4)
    h_pass(5)
    up(7)
    up_send(7)
    early = len(sent)
    sum_over_cores()
    down(5)
    h_pass(6)
    down(1)
    down(6)
    down(2)
    down(3)
    loads["rweights"].wait()
    combine_weights()
    h_pass(7)
    down(7)

    for copy in sent[:early]:
        copy.wait_send()
    split = ep // 2
    for k in range(1, split):
        arrived(rbuf.at[block(k)], b_send.at[k], b_recv.at[k], pair(k))

    def weighed(cols):
        rows_back = rbuf[cols, :]
        return dot(w_hi[:, cols], rows_back) + dot(w_lo[:, cols], rows_back)

    close = weighed(block(0, split))
    total = part[t].astype(F32) + rs1[y].astype(F32)
    for a in range(1, ys):
        arrived(rs2_recv.at[a - 1], r2_send.at[a - 1], r2_recv.at[a - 1], over_y(a))
        total += rs2_recv[a - 1].astype(F32)
    ret_out[...] = total.astype(BF16)
    for copy in sent[early:]:
        copy.wait_send()
    for k in range(split, ep):
        arrived(rbuf.at[block(k)], b_send.at[k], b_recv.at[k], pair(k))
    exp_out[...] = (close + weighed(block(split, ep - split))).astype(BF16)

    @pl.when(bit(last) == 0)
    def _():
        state_copy(last).wait_send()


def body(
    query_in, key_in, value_in, gate_in, decay_rate, head_gain, output_weight,
    token_rows, token_gain, route_ids, route_weights, expert_gate, expert_up, expert_down,
):
    ep, tp = lax.axis_size("ep"), lax.axis_size("tp")
    tokens, model = token_rows.shape
    top = route_ids.shape[1]
    cap = -(-(2 * tokens * top // ep) // 32) * 32
    block_len, width = query_in.shape
    heads = decay_rate.shape[0]
    dk = width // heads
    ff = expert_gate.shape[2]
    cw = expert_down.shape[2]
    ys = tp // 2
    rounds = ep.bit_length() - 1
    assert ep == 2**rounds and rounds >= 3
    per = ep // UNITS
    pieces = max(1, min(PIECES, model // (2 * 128 * ys)))
    turns = dk // 2
    freq = np.tile(
        np.float32(rope_base) ** (-np.arange(turns, dtype=np.float32) * np.float32(2.0 / dk)), 2)
    turn_sign = np.where(np.arange(dk) < turns, -1.0, 1.0)
    size = dict(ep=ep, tp=tp, cap=cap, rounds=rounds, per=per, groups=GROUPS, pieces=pieces)
    slots = ep * cap
    rb = block_len // tp
    hbm = pl.BlockSpec(memory_space=pl.ANY)
    vmem = pl.BlockSpec(memory_space=pltpu.VMEM)
    dma = pltpu.SemaphoreType.DMA
    given = [
        route_ids.T, token_rows, token_gain[None, :], expert_gate[0], expert_up[0],
        query_in, key_in, value_in, decay_rate,
        jnp.asarray(freq[None, :], F32), jnp.asarray(turn_sign[None, :], F32),
        route_weights.T, gate_in, head_gain[None, :], output_weight, expert_down[0],
    ]
    nm = len(GROUPS)
    outs = pl.pallas_call(
        functools.partial(kernel, size),
        out_shape=(pltpu.VMEM((rb, model), BF16), pltpu.VMEM((tokens, cw), BF16)),
        in_specs=[hbm] * len(given),
        out_specs=(vmem, vmem),
        scratch_shapes=[
            (pltpu.SMEM if a is decay_rate else pltpu.VMEM)(a.shape, a.dtype) for a in given]
        + [
            pltpu.VMEM((tokens, model), BF16),
            pltpu.VMEM((tokens, model // 2), BF16),
            pltpu.VMEM((top, tokens), jnp.int32),
            pltpu.VMEM((slots // 2, tokens), BF16),
            pltpu.VMEM((slots, model // 2), BF16),
            pltpu.VMEM((2, slots, model // 2), BF16),
            pltpu.VMEM((tp, slots, ff), BF16),
            pltpu.VMEM((per * cap, ff), F32),
            pltpu.VMEM((per * cap, ff), F32),
            pltpu.VMEM((slots, cw), BF16),
            pltpu.VMEM((slots, cw), BF16),
            pltpu.VMEM((tokens, slots), BF16),
            pltpu.VMEM((tokens, slots), BF16),
            pltpu.VMEM((block_len, dk), F32),
            pltpu.VMEM((block_len, dk), F32),
            pltpu.VMEM((block_len, width), BF16),
            pltpu.VMEM((block_len, width), BF16),
            pltpu.VMEM((block_len, width), F32),
            pltpu.VMEM((heads, dk, dk), F32),
            pltpu.VMEM((heads, dk, dk), F32),
            pltpu.VMEM((rounds, heads, dk, dk), BF16),
            pltpu.VMEM((rounds, heads, dk, dk), BF16),
            pltpu.VMEM((block_len, width), BF16),
            pltpu.VMEM((tp, rb, model), BF16),
            pltpu.VMEM((ys, rb, model), BF16),
            pltpu.VMEM((max(ys - 1, 1), rb, model), BF16),
            pltpu.VMEM((max(ys - 1, 1), rb, model), BF16),
            dma((len(given) + 2,)),
            dma((1,)), dma((1,)), dma((pieces,)), dma((pieces,)),
            dma((ys, pieces)), dma((ys, pieces)),
            dma((ep, pieces)), dma((ep, pieces)),
            dma((UNITS,)), dma((UNITS,)),
            dma((ys, nm)), dma((ys, nm)), dma((ys, nm)), dma((ys, nm)),
            dma((ep,)), dma((ep,)),
            dma((rounds,)), dma((rounds,)),
            dma((ys,)), dma((ys,)), dma((ys,)), dma((ys,)),
        ],
        compiler_params=pltpu.CompilerParams(
            collective_id=0, has_side_effects=True, vmem_limit_bytes=VMEM_LIMIT
        ),
    )(*given)
    return outs


def solution(mesh):
    placed = (
        P("ep", "tp"), P("ep", "tp"), P("ep", "tp"), P("ep", "tp"),
        P("tp"), P("tp"), P("tp", None), P("ep", None), P(),
        P("ep", None), P("ep", None),
        P("ep", None, "tp"), P("ep", None, "tp"), P("ep", None, "tp"),
    )
    return jax.shard_map(
        body,
        mesh=mesh,
        in_specs=placed,
        out_specs=(P(("ep", "tp"), None), P("ep", "tp")),
        check_vma=False,
    )
```
